512 devices in a mesh: sp: 16 (over z), fs: 4 (over y), tp: 8 (over x, core).
Axes of the slice: x: 4, y: 4, z: 16, core: 2. Of those that a mesh axis runs over, the one named last changes fastest.
Arguments:
- tokens: bfloat16 [4, 8192, 2048], P('fs', ('sp', 'tp')), may hold values from -6 to 6
- input_gain: float32 [2048], replicated, may hold values from 0.1 to 1.9
- query_weight: bfloat16 [2048, 768], P(None, 'tp'), may hold values from -0.125 to 0.125
- latent_down: bfloat16 [2048, 256], replicated, may hold values from -0.125 to 0.125
- rotary_down: bfloat16 [2048, 32], replicated, may hold values from -0.125 to 0.125
- pool_down: bfloat16 [2048, 1024], P(None, 'tp'), may hold values from -0.125 to 0.125
- key_up: bfloat16 [256, 512], replicated, may hold values from -0.375 to 0.375
- value_up: bfloat16 [256, 1024], replicated, may hold values from -1.125 to 1.125, as said below
- query_gain: float32 [96], replicated, may hold values from 0.1 to 1.9
- key_gain: float32 [96], replicated, may hold values from 0.1 to 1.9
- pool_weight: bfloat16 [16, 64, 64], replicated, may hold values from -2.25 to 2.25, as said below
- pool_scale: float32 [1024], P('tp'), may hold values from 0.1 to 1.9
- attention_gain: float32 [1024], P('tp'), may hold values from 0.1 to 1.9
- pool_gain: float32 [1024], P('tp'), may hold values from 0.1 to 1.9
- attention_out: bfloat16 [1024, 2048], P('tp'), may hold values from -0.125 to 0.125
- pool_out: bfloat16 [1024, 2048], P('tp'), may hold values from -0.125 to 0.125
Outputs:
- mixed: bfloat16 [4, 8192, 2048], P('fs', ('sp', 'tp'))
The draws below stay inside these ranges and needn't reach their ends.
Inputs may be any that keep to these rules, and one draw needn't show every extreme that they name: `value_up`: entries of order 256 ** -0.5 or larger. `pool_weight`: entries of order 64 ** -0.5 or larger.
All inputs are finite; a program needn't handle non-finite values.
Results may differ from the reference program's by a relative error of at most 0.015.
Values may be sent and summed in bfloat16 or wider, within the bound.
A program may use at most 64 MiB of HBM per device.

```python
import math
import jax
import jax.numpy as jnp
from jax import lax

D = 2048
HEADS = 8
NOPE_DIM = 64
ROPE_DIM = 32
VALUE_DIM = 128
KV_LATENT = 256
GROUPS = 16
GROUP_DIM = 64
QK_DIM = 96
POOL_WIDTH = 1024
SEQS = 4
LENGTH = 8192
HEAD_BLOCKS = 8


def draw_value_up(key, part):
    columns = jnp.arange(HEADS * VALUE_DIM, dtype=jnp.int32) // VALUE_DIM
    level = columns.astype(jnp.float32) / (HEADS - 1)
    base = jnp.clip(jax.random.normal(key, (KV_LATENT, HEADS * VALUE_DIM), jnp.float32), -6.0, 6.0)
    factor = 3.0 ** level
    return (base * factor[None, :] * KV_LATENT ** (-0.5)).astype(jnp.bfloat16)


def draw_pool_weight(key, part):
    level = jnp.arange(GROUPS, dtype=jnp.int32).astype(jnp.float32) / (GROUPS - 1)
    base = jnp.clip(jax.random.normal(key, (GROUPS, GROUP_DIM, GROUP_DIM), jnp.float32), -6.0, 6.0)
    factor = 3.0 ** level
    return (base * factor[:, None, None] * GROUP_DIM ** (-0.5)).astype(jnp.bfloat16)


def steps_of(stream_key, shape, split, least, high):
    def one(position, blocks):
        draws = jax.random.uniform(jax.random.fold_in(jax.random.fold_in(stream_key, 6), position), (blocks,), jnp.float32, least / len(split), high / len(split))
        return jnp.repeat(jnp.exp(draws), shape[position] // blocks).reshape((-1,) + (1,) * (len(shape) - position - 1))

    factor_of = one(*split[0])
    for cut in split[1:]:
        factor_of = factor_of * one(*cut)
    return factor_of


def centred(key, extent, deviation, bound, pieces=(), kind=jnp.bfloat16):
    entries = deviation * jax.random.normal(key, extent, jnp.float32)
    if pieces:
        entries = entries * steps_of(key, extent, pieces, -0.22, 0.18)
    return jnp.clip(entries, -bound, bound).astype(kind)


def setup_inputs(seed: int = 0) -> dict:
    streams_of = jax.random.split(jax.random.key(seed), 17)
    tokens = centred(streams_of[0], (SEQS, LENGTH, D), 1.0, 6.0, ((0, 4), (1, 128)))
    input_gain = jnp.clip(1.0 + 0.18 * jax.random.normal(streams_of[1], (D,), jnp.float32), 0.1, 1.9)
    query_weight = centred(streams_of[2], (D, HEADS * QK_DIM), D ** -0.5, 0.125, ((1, 8),))
    latent_down = centred(streams_of[3], (D, KV_LATENT), D ** -0.5, 0.125)
    rotary_down = centred(streams_of[4], (D, ROPE_DIM), D ** -0.5, 0.125)
    pool_down = centred(streams_of[5], (D, POOL_WIDTH), D ** -0.5, 0.125, ((1, 8),))
    key_up = centred(streams_of[6], (KV_LATENT, HEADS * NOPE_DIM), KV_LATENT ** -0.5, 0.375)
    value_up = draw_value_up(jax.random.fold_in(streams_of[16], 71), 0)
    query_gain = jnp.clip(1.0 + 0.18 * jax.random.normal(streams_of[8], (QK_DIM,), jnp.float32), 0.1, 1.9)
    key_gain = jnp.clip(1.0 + 0.18 * jax.random.normal(streams_of[9], (QK_DIM,), jnp.float32), 0.1, 1.9)
    pool_weight = draw_pool_weight(jax.random.fold_in(streams_of[16], 71), 0)
    pool_scale = jnp.clip(1.0 + 0.18 * jax.random.normal(streams_of[11], (POOL_WIDTH,), jnp.float32), 0.1, 1.9)
    attention_gain = jnp.clip(1.0 + 0.18 * jax.random.normal(streams_of[12], (HEADS * VALUE_DIM,), jnp.float32), 0.1, 1.9)
    pool_gain = jnp.clip(1.0 + 0.18 * jax.random.normal(streams_of[13], (POOL_WIDTH,), jnp.float32), 0.1, 1.9)
    attention_out = centred(streams_of[14], (HEADS * VALUE_DIM, D), (HEADS * VALUE_DIM + POOL_WIDTH) ** -0.5, 0.125, ((0, 8),))
    pool_out = centred(streams_of[15], (POOL_WIDTH, D), (HEADS * VALUE_DIM + POOL_WIDTH) ** -0.5, 0.125, ((0, 8),))
    return {"tokens": tokens, "input_gain": input_gain, "query_weight": query_weight, "latent_down": latent_down, "rotary_down": rotary_down, "pool_down": pool_down, "key_up": key_up, "value_up": value_up, "query_gain": query_gain, "key_gain": key_gain, "pool_weight": pool_weight, "pool_scale": pool_scale, "attention_gain": attention_gain, "pool_gain": pool_gain, "attention_out": attention_out, "pool_out": pool_out}


EPS = 1e-06
THETA = 10000.0
rim_rows = 16

def rms_scale(values):
    return lax.rsqrt(lax.optimization_barrier(jnp.mean(values * values, axis=-1, keepdims=True)) + EPS)

def rotate(values, positions):
    half = values.shape[-1] // 2
    inv_freq = 1.0 / THETA ** (jnp.arange(half, dtype=jnp.float32) / half)
    angle = positions[:, None, None] * inv_freq
    cosine = jnp.cos(angle)
    sine = jnp.sin(angle)
    first = values[..., :half]
    second = values[..., half:]
    return jnp.concatenate([first * cosine - second * sine, second * cosine + first * sine], axis=-1)

def head_vectors(raw, gain, positions):
    normal = raw * rms_scale(raw) * gain
    turned = rotate(normal[..., NOPE_DIM:], positions)
    return jnp.concatenate([normal[..., :NOPE_DIM], turned], axis=-1).astype(jnp.bfloat16)

def expand_keys(latent_rows, first, key_up, value_up, key_gain):
    count = latent_rows.shape[0]
    heads = key_up.shape[1] // NOPE_DIM
    latent = latent_rows[:, :KV_LATENT].astype(jnp.float32)
    latent_normed = (latent * rms_scale(latent)).astype(jnp.bfloat16)
    plain = jnp.dot(latent_normed, key_up, preferred_element_type=jnp.float32).reshape(count, heads, NOPE_DIM)
    values = jnp.dot(latent_normed, value_up, preferred_element_type=jnp.float32).astype(jnp.bfloat16)
    shared = latent_rows[:, KV_LATENT:].astype(jnp.float32)
    shared = jnp.broadcast_to(shared[:, None, :], (count, heads, ROPE_DIM))
    positions = (first + jnp.arange(count, dtype=jnp.int32)).astype(jnp.float32)
    keys = head_vectors(jnp.concatenate([plain, shared], axis=-1), key_gain, positions)
    return (keys, values.reshape(count, heads, VALUE_DIM))

def pool_mix(pool_input, before, group_ids, positions):
    count = pool_input.shape[0]
    groups = group_ids.shape[0]
    current = pool_input.astype(jnp.float32).reshape(count, groups, GROUP_DIM)
    extended = jnp.concatenate([before, pool_input], axis=0).astype(jnp.float32)
    extended = extended.reshape(count + rim_rows, groups, GROUP_DIM)
    window = jnp.left_shift(2, group_ids % 4).astype(jnp.float32)
    total = current
    for back in range(1, rim_rows):
        taken = (window > back).astype(jnp.float32)
        total = total + extended[rim_rows - back:rim_rows - back + count] * taken[None, :, None]
    divisor = jnp.minimum(positions[:, None] + 1.0, window[None, :])
    return (total / divisor[:, :, None] - current).astype(jnp.bfloat16)

def one_sequence(tokens, input_gain, query_weight, latent_down, rotary_down, pool_down, key_up, value_up, query_gain, key_gain, pool_weight, pool_scale, attention_gain, pool_gain, attention_out, pool_out):
    count = tokens.shape[0]
    source = tokens.astype(jnp.float32)
    normed = (source * rms_scale(source) * input_gain).astype(jnp.bfloat16)
    latent_rows = jnp.concatenate([jnp.dot(normed, latent_down, preferred_element_type=jnp.float32), jnp.dot(normed, rotary_down, preferred_element_type=jnp.float32)], axis=1).astype(jnp.bfloat16)
    query_raw = jnp.dot(normed, query_weight, preferred_element_type=jnp.float32).reshape(count, HEADS, QK_DIM)
    pool_input = jnp.dot(normed, pool_down, preferred_element_type=jnp.float32).astype(jnp.bfloat16)
    positions_int = jnp.arange(count, dtype=jnp.int32)
    positions = positions_int.astype(jnp.float32)
    queries = lax.optimization_barrier(head_vectors(query_raw, query_gain, positions)).astype(jnp.float32)
    keys, values = expand_keys(latent_rows, 0, key_up, value_up, key_gain)
    keys = lax.optimization_barrier(keys).astype(jnp.float32)
    values = lax.optimization_barrier(values).astype(jnp.float32)
    factor = 1.0 / math.sqrt(QK_DIM)
    qblock = math.gcd(count, 512)

    def attend_block(index):
        begin = index * qblock
        query_block = lax.dynamic_slice_in_dim(queries, begin, qblock, 0)
        scores = jnp.einsum('qhd,khd->hqk', query_block, keys) * factor
        query_pos = begin + jnp.arange(qblock, dtype=jnp.int32)
        visible = positions_int[None, None, :] <= query_pos[None, :, None]
        weights = jnp.where(visible, jnp.exp(scores), 0.0)
        rounded = lax.optimization_barrier(weights.astype(jnp.bfloat16)).astype(jnp.float32)
        numer = jnp.einsum('hqk,khd->qhd', rounded, values)
        denom = lax.optimization_barrier(jnp.sum(weights, axis=-1))
        return numer / jnp.transpose(denom)[:, :, None]
    attended = lax.map(attend_block, jnp.arange(count // qblock, dtype=jnp.int32))
    attended = attended.reshape(count, HEADS * VALUE_DIM)
    before = jnp.zeros((rim_rows, POOL_WIDTH), jnp.bfloat16)
    pooled_mean = pool_mix(pool_input, before, jnp.arange(GROUPS, dtype=jnp.int32), positions)
    pooled = jnp.einsum('rgc,gcd->rgd', pooled_mean.astype(jnp.float32), pool_weight.astype(jnp.float32))
    pooled = pooled.reshape(count, POOL_WIDTH) * pool_scale
    attention_mixed = (attended * rms_scale(attended) * attention_gain).astype(jnp.bfloat16)
    pool_mixed = (pooled * rms_scale(pooled) * pool_gain).astype(jnp.bfloat16)
    head_cols = HEADS * VALUE_DIM // HEAD_BLOCKS
    pool_cols = POOL_WIDTH // HEAD_BLOCKS
    total = jnp.zeros((count, D), jnp.float32)
    for member in range(HEAD_BLOCKS):
        term = jnp.dot(attention_mixed[:, member * head_cols:(member + 1) * head_cols], attention_out[member * head_cols:(member + 1) * head_cols], preferred_element_type=jnp.float32)
        term = term + jnp.dot(pool_mixed[:, member * pool_cols:(member + 1) * pool_cols], pool_out[member * pool_cols:(member + 1) * pool_cols], preferred_element_type=jnp.float32)
        total = total + lax.optimization_barrier(term.astype(jnp.bfloat16)).astype(jnp.float32)
    return total.astype(jnp.bfloat16)

def reference(tokens, input_gain, query_weight, latent_down, rotary_down, pool_down, key_up, value_up, query_gain, key_gain, pool_weight, pool_scale, attention_gain, pool_gain, attention_out, pool_out):
    results = []
    for sequence in range(SEQS):
        results.append(one_sequence(tokens[sequence], input_gain, query_weight, latent_down, rotary_down, pool_down, key_up, value_up, query_gain, key_gain, pool_weight, pool_scale, attention_gain, pool_gain, attention_out, pool_out))
    return jnp.stack(results)
```

```python
import functools
import math

import jax
import jax.numpy as jnp
import numpy as np
from jax import lax
from jax.experimental import pallas as pl
from jax.experimental.pallas import tpu as pltpu
from jax.sharding import PartitionSpec as P

MESH = pl.DeviceIdType.MESH
BF = jnp.bfloat16
F32 = jnp.float32

EPS = 1e-06
THETA = 10000.0
QK = 96
SCALE = math.log2(math.e) / math.sqrt(QK)
NX = 4
NS = 16
BLOCK = 512
ROWS = 64
RIM = 16
UP = (0, 3, 2)
DOWN = (0, 1, 2)


def dot(a, b, dims=((1,), (0,)), precision=None):
    return lax.dot_general(a, b, (dims, ((), ())), preferred_element_type=F32, precision=precision)


def kernel(
    tokens, ig, qw, ld, rd, pd, ku, vu, qg, kg, pw, ps, ag, pg, ao, po, tab,
    out,
    tokv, nt, qwv, ldv, rdv, pdv, kuv, vuv, pwv, w2, tabv,
    xt, kut, vut, qv, ktv, vtv, acc, qcol, kcol, rim, halo, poolin, px, ax, bpart,
    ssq, part, far, fin, ownp, fcol,
    dsem, usnd, urcv, dsnd, drcv, ysnd, yrcv, gsnd, grcv, osnd, orcv, psnd, prcv,
    tsnd, trcv, vsnd, vrcv, wsnd, wrcv, hsnd, hrcv, esnd, ercv, ssnd, srcv, rsnd, rrcv,
):
    z = lax.axis_index("sp")
    fs = lax.axis_index("fs")
    p = lax.axis_index("tp")
    c = lax.rem(p, 2)
    x = p // 2
    o = 1 - c

    def zmod(v):
        return lax.rem(v + 2 * NS, NS)

    def xmod(v):
        return lax.rem(v + 2 * NX, NX)

    def at(zz, xx, cc):
        return (zz, fs, xx * 2 + cc)

    xr, xl, xf = xmod(x + 1), xmod(x - 1), xmod(x + 2)
    zu, zd = zmod(z + 1), zmod(z - 1)

    def send(src, dst, ssem, rsem, dev):
        copy = pltpu.make_async_remote_copy(
            src_ref=src, dst_ref=dst, send_sem=ssem, recv_sem=rsem, device_id=dev, device_id_type=MESH
        )
        copy.start()

    def got(dst, ssem, rsem):
        pltpu.make_async_remote_copy(
            src_ref=dst, dst_ref=dst, send_sem=ssem, recv_sem=rsem,
            device_id=at(z, x, o), device_id_type=MESH,
        ).wait_recv()

    def sent(src, ssem, rsem):
        pltpu.make_async_remote_copy(
            src_ref=src, dst_ref=src, send_sem=ssem, recv_sem=rsem,
            device_id=at(z, x, o), device_id_type=MESH,
        ).wait_send()

    half = out.shape[2] // 2
    mine = pl.ds(pl.multiple_of(c * half, 128), half)
    theirs = pl.ds(pl.multiple_of(o * half, 128), half)
    kcols = pl.ds(pl.multiple_of(x * 128, 128), 128)
    vcols = pl.ds(pl.multiple_of(p * 128, 128), 128)
    wrows = pl.ds(pl.multiple_of(c * 128, 128), 128)
    loads = [
        (tokens.at[0], tokv),
        (ld, ldv),
        (rd, rdv),
        (qw, qwv),
        (pd, pdv),
        (ku.at[:, kcols], kuv),
        (vu.at[:, vcols], vuv),
        (pw.at[pl.ds(p * 2, 2)], pwv),
        (tab, tabv),
        (ao.at[:, mine], w2.at[0, wrows]),
        (po.at[:, mine], w2.at[1, wrows]),
    ]
    copies = [pltpu.make_async_copy(s, d, dsem.at[i]) for i, (s, d) in enumerate(loads)]
    for copy in copies:
        copy.start()

    barrier = pltpu.get_barrier_semaphore()
    peers = [at(z, x, o), at(zu, x, c), at(zd, x, c)]
    peers += [at(z, xx, cc) for xx in (xr, xl, xf) for cc in (c, o)]
    for peer in peers:
        pl.semaphore_signal(barrier, inc=1, device_id=peer, device_id_type=MESH)

    copies[0].wait()
    source = tokv[...].astype(F32)
    scale = lax.rsqrt(jnp.mean(source * source, axis=1, keepdims=True) + EPS)
    normed = (source * scale * ig[...]).astype(BF)
    nt[p] = normed
    copies[1].wait()
    copies[2].wait()
    latent = dot(normed, ldv[...]).astype(BF).astype(F32)
    rotary = dot(normed, rdv[...]).astype(BF).astype(F32)
    lat = latent * lax.rsqrt(jnp.mean(latent * latent, axis=1, keepdims=True) + EPS)
    stacked = jnp.concatenate([lat[:, :128], lat[:, 128:]], axis=0)
    turned = jnp.concatenate([rotary[:, :16], rotary[:, 16:32]], axis=0)
    xt[z, c, x, 0:128, :] = stacked.T.astype(BF)
    xt[z, c, x, 128:144, :] = turned.T.astype(BF)

    pl.semaphore_wait(barrier, len(peers))

    own = xt.at[z, c, x]

    def up(s, k, piece):
        send(piece, piece, usnd.at[s, k], urcv.at[s, k], at(zu, x, c))

    def down(s, k, piece):
        send(piece, piece, dsnd.at[s, k], drcv.at[s, k], at(zd, x, c))

    def other(sem, r, piece):
        send(piece, piece, osnd.at[sem, r], orcv.at[sem, r], at(z, x, o))

    send(own, own, gsnd.at[0], grcv.at[0], at(z, xr, c))
    send(own, own, gsnd.at[1], grcv.at[1], at(z, xl, c))
    up(0, 0, own)
    down(0, 0, own)
    send(own, own, gsnd.at[2], grcv.at[2], at(z, xf, c))
    other(15, 0, own)

    hrows = ROWS // 2

    def trows(xx, h):
        return nt.at[xx * 2 + c, pl.ds(h * hrows, hrows)]

    for h in (0, 1):
        send(trows(x, h), trows(x, h), tsnd.at[0, h], trcv.at[0, h], at(z, xr, c))
        send(trows(x, 1 - h), trows(x, 1 - h), tsnd.at[1, 1 - h], trcv.at[1, 1 - h], at(z, xl, c))
    send(nt.at[p], nt.at[p], vsnd.at[0], vrcv.at[0], at(z, x, o))

    for i, w in enumerate((ao, po)):
        send(w.at[:, theirs], w2.at[i, wrows], wsnd.at[i], wrcv.at[i], at(z, x, o))

    copies[5].wait()
    copies[6].wait()
    kut[...] = kuv[...].astype(F32).T.astype(BF)
    vut[...] = vuv[...].astype(F32).T.astype(BF)
    qcol[...] = jnp.broadcast_to(qg[...], (128, QK)).T
    kcol[...] = jnp.broadcast_to(kg[...], (128, QK)).T
    vtv[128:256, :] = jnp.ones((128, BLOCK), BF)
    ktv[QK:128, :] = jnp.zeros((128 - QK, BLOCK), BF)
    acc[...] = jnp.zeros_like(acc)

    for sem, rel in ((1, 1), (0, 3), (2, 2)):
        piece = xt.at[z, c, xmod(x + rel)]
        got(piece, gsnd.at[sem], grcv.at[sem])
        if rel in UP:
            up(0, UP.index(rel), piece)
        if rel in DOWN:
            down(0, DOWN.index(rel), piece)
        other(15, rel, piece)

    copies[8].wait()

    def rotate(a, b, first):
        cosine = tabv[0:16, pl.ds(first, a.shape[1])]
        sine = tabv[16:32, pl.ds(first, a.shape[1])]
        return a * cosine - b * sine, b * cosine + a * sine

    def expand(j):
        lane = lax.broadcasted_iota(jnp.int32, (144, 128), 1)
        low, high = [], []
        for xx in range(NX):
            p0 = xt[j, 0, xx].astype(F32)
            p1 = xt[j, 1, xx].astype(F32)
            low.append(jnp.where(lane < 64, p0, pltpu.roll(p1, 64, 1)))
            high.append(jnp.where(lane < 64, pltpu.roll(p0, 64, 1), p1))
        low = jnp.concatenate(low, axis=1)
        high = jnp.concatenate(high, axis=1)
        lat2 = jnp.concatenate([low[:128].astype(BF), high[:128].astype(BF)], axis=0)
        plain = dot(kut[pl.ds(pl.multiple_of(c * 64, 64), 64), :], lat2)
        vtv[0:128, :] = dot(vut[...], lat2).astype(BF)
        a, b = low[128:144], high[128:144]
        total = jnp.sum(plain * plain, axis=0, keepdims=True)
        total = total + jnp.sum(a * a + b * b, axis=0, keepdims=True)
        factor = lax.rsqrt(total * (1.0 / QK) + EPS)
        gain = kcol[:, 0:1]
        first = pl.multiple_of(j * BLOCK, 128)
        a, b = rotate(a * factor * gain[64:80], b * factor * gain[80:96], first)
        ktv[0:64, :] = (plain * factor * gain[0:64]).astype(BF)
        ktv[64:80, :] = a.astype(BF)
        ktv[80:96, :] = b.astype(BF)

    def attend(masked):
        for i in range(2):
            rows = pl.ds(i * 256, 256)
            weight = jnp.exp2(dot(qv[rows, :], ktv[...]))
            if masked:
                qpos = lax.broadcasted_iota(jnp.int32, weight.shape, 0) + i * 256
                kpos = lax.broadcasted_iota(jnp.int32, weight.shape, 1)
                weight = jnp.where(kpos <= qpos, weight, 0.0)
            acc[rows, :] += dot(weight.astype(BF), vtv[...], ((1,), (1,)))

    def unit(u):
        odd = lax.rem(u, 2)
        j = jnp.where(odd == 1, z - (u + 1) // 2, z + u // 2 - NS)

        @pl.when(j >= 0)
        def _():
            expand(j)
            attend(False)

    def project():
        first = pl.multiple_of(z * BLOCK, 128)

        def chunk(t, carry):
            rows = jnp.concatenate([nt[2 * t], nt[2 * t + 1]], axis=0)
            spot = pl.ds(pl.multiple_of(t * 128, 128), 128)
            poolin[pl.ds(pl.multiple_of(t * 128 + RIM, 8), 128), :] = (
                dot(rows, pdv[...]).astype(BF).astype(F32)
            )
            raw = dot(rows, qwv[...]).T
            total = jnp.sum(raw * raw, axis=0, keepdims=True)
            normal = raw * lax.rsqrt(total * (1.0 / QK) + EPS) * qcol[:, 0:1] * SCALE
            a, b = rotate(normal[64:80], normal[80:96], pl.multiple_of(first + t * 128, 128))
            full = jnp.concatenate([normal[:64], a, b, jnp.zeros((32, 128), F32)], axis=0)
            qv[spot, :] = full.T.astype(BF)
            return carry

        lax.fori_loop(0, NX, chunk, 0)
        rim[...] = poolin[BLOCK:, :].astype(BF)
        send(rim, halo, hsnd.at[0], hrcv.at[0], at(zu, x, c))

    def sumsq(values):
        return dot(jnp.ones((8, 128), F32), values * values, ((1,), (1,)), lax.Precision.HIGHEST)

    def spread(totals, start):
        sub = lax.broadcasted_iota(jnp.int32, (8, 128), 0)
        packed = jnp.zeros((8, 128), F32)
        for t in range(NX):
            packed = jnp.where(sub == start + t, totals[:, t * 128 : (t + 1) * 128], packed)
        return packed

    def pool():
        got(halo, hsnd.at[0], hrcv.at[0])
        poolin[0:RIM, :] = jnp.where(z > 0, halo[...].astype(F32), 0.0)
        values = poolin[...]
        two = values + pltpu.roll(values, 1, 0)
        four = two + pltpu.roll(two, 2, 0)
        eight = four + pltpu.roll(four, 4, 0)
        sixteen = eight + pltpu.roll(eight, 8, 0)
        lane = lax.broadcasted_iota(jnp.int32, (BLOCK, 128), 1)
        wide = c == 1
        left = jnp.where(wide ^ (x < 0), eight, two)[RIM:]
        right = jnp.where(wide ^ (x < 0), sixteen, four)[RIM:]
        total = jnp.where(lane < 64, left, right)
        base = jnp.where(wide, 8.0, 2.0)
        window = jnp.where(lane < 64, base, base * 2.0)
        count = (lax.broadcasted_iota(jnp.int32, (BLOCK, 128), 0) + (z * BLOCK + 1)).astype(F32)
        mean = (total / jnp.minimum(count, window) - values[RIM:]).astype(BF)
        zero = jnp.zeros((64, 64), F32)
        w0 = jnp.concatenate([pwv[0].astype(F32), zero], axis=1)
        w1 = jnp.concatenate([zero, pwv[1].astype(F32)], axis=1)
        pooled = dot(mean, jnp.concatenate([w0, w1], axis=0).astype(BF)) * ps[...]
        ssq[p] = spread(sumsq(pooled), 4)
        px[c] = (pooled * pg[...]).astype(BF)
        send(px.at[c], px.at[c], psnd.at[0], prcv.at[0], at(z, x, o))

    def project_pool():
        got(px.at[o], psnd.at[0], prcv.at[0])
        for i in (0, 1):
            copies[9 + i].wait()
            got(w2.at[i, pl.ds(pl.multiple_of(o * 128, 128), 128)], wsnd.at[i], wrcv.at[i])

        def chunk(t, carry):
            rows = pl.ds(pl.multiple_of(t * 128, 128), 128)
            both = jnp.concatenate([px[0, rows], px[1, rows]], axis=1)
            for h in (0, 1):
                bpart[t, h] = dot(both, w2[1, :, h * 512 : (h + 1) * 512])
            return carry

        lax.fori_loop(0, NX, chunk, 0)

    def step(s, carry):
        ju, jd = zmod(z - s), zmod(z + s)
        for k in range(3):
            piece = xt.at[ju, c, xmod(x + UP[k])]
            got(piece, usnd.at[s - 1, k], urcv.at[s - 1, k])

            @pl.when(s < 8)
            def _():
                up(s, k, piece)

            other(2 * s - 2, UP[k], piece)
            if UP[k] == 0:
                send(piece, piece, ysnd.at[0, s - 1], yrcv.at[0, s - 1], at(z, xl, c))

            @pl.when(s < 8)
            def _():
                piece = xt.at[jd, c, xmod(x + DOWN[k])]
                got(piece, dsnd.at[s - 1, k], drcv.at[s - 1, k])

                @pl.when(s < 7)
                def _():
                    down(s, k, piece)

                other(2 * s - 1, DOWN[k], piece)
                if DOWN[k] == 0:
                    send(piece, piece, ysnd.at[1, s - 1], yrcv.at[1, s - 1], at(z, xr, c))

        @pl.when(s >= 2)
        def _():
            sides(s - 1, True)

        @pl.when(s >= 3)
        def _():
            arrived(s - 2, True)

        @pl.when(s == 1)
        def _():
            got(trows(xl, 0), tsnd.at[0, 0], trcv.at[0, 0])
            send(trows(xl, 0), trows(xl, 0), tsnd.at[0, 2], trcv.at[0, 2], at(z, xr, c))
            got(trows(xr, 1), tsnd.at[1, 1], trcv.at[1, 1])
            send(trows(xr, 1), trows(xr, 1), tsnd.at[1, 2], trcv.at[1, 2], at(z, xl, c))

        @pl.when(s == 2)
        def _():
            got(trows(xl, 1), tsnd.at[0, 1], trcv.at[0, 1])
            got(trows(xr, 0), tsnd.at[1, 0], trcv.at[1, 0])
            for i, xx in ((1, xl), (2, xr)):
                block = nt.at[xx * 2 + c]
                send(block, block, vsnd.at[i], vrcv.at[i], at(z, x, o))

        @pl.when(s == 3)
        def _():
            got(trows(xf, 0), tsnd.at[0, 2], trcv.at[0, 2])
            got(trows(xf, 1), tsnd.at[1, 2], trcv.at[1, 2])
            block = nt.at[xf * 2 + c]
            send(block, block, vsnd.at[3], vrcv.at[3], at(z, x, o))

        @pl.when(s == 4)
        def _():
            for i, xx in ((0, x), (1, xl), (2, xr), (3, xf)):
                got(nt.at[xx * 2 + o], vsnd.at[i], vrcv.at[i])
            copies[3].wait()
            copies[4].wait()
            project()
            for r in range(4):
                got(xt.at[z, o, xmod(x + r)], osnd.at[15, r], orcv.at[15, r])
            expand(z)
            attend(True)

        @pl.when(s == 5)
        def _():
            copies[7].wait()
            pool()

        @pl.when(s == 6)
        def _():
            project_pool()

        def limit(v):
            return jnp.maximum(jnp.minimum(3 * (v - 4) + 2, 2 * (v - 2)), 0)

        def run(u, carry):
            unit(u)
            return carry

        lax.fori_loop(limit(s - 1) + 1, limit(s) + 1, run, 0)
        return carry

    def sides(s, below):
        piece = xt.at[zmod(z - s), c, xr]
        got(piece, ysnd.at[0, s - 1], yrcv.at[0, s - 1])
        other(2 * s - 2, 1, piece)
        if below:
            piece = xt.at[zmod(z + s), c, xl]
            got(piece, ysnd.at[1, s - 1], yrcv.at[1, s - 1])
            other(2 * s - 1, 3, piece)

    def arrived(s, below):
        for r in range(4):
            got(xt.at[zmod(z - s), o, xmod(x + r)], osnd.at[2 * s - 2, r], orcv.at[2 * s - 2, r])
            if below:
                got(xt.at[zmod(z + s), o, xmod(x + r)], osnd.at[2 * s - 1, r], orcv.at[2 * s - 1, r])

    lax.fori_loop(1, 9, step, 0)
    sides(8, False)
    arrived(7, True)
    arrived(8, False)

    def last(u, carry):
        unit(u)
        return carry

    lax.fori_loop(13, 16, last, 0)

    attended = acc[:, :128] / acc[:, 128:]
    ssq[p] = ssq[p] + spread(sumsq(attended), 0)
    ax[c] = (attended * ag[...]).astype(BF)
    send(ax.at[c], ax.at[c], psnd.at[1], prcv.at[1], at(z, x, o))
    tpeers = [(0, xr, c), (1, xr, o), (2, xl, c), (3, xl, o), (4, xf, c), (5, xf, o), (6, x, o)]
    for i, xx, cc in tpeers:
        send(ssq.at[p], ssq.at[p], ssnd.at[i], srcv.at[i], at(z, xx, cc))
    got(ax.at[o], psnd.at[1], prcv.at[1])
    spots = [(0, xl, c), (1, xl, o), (2, xr, c), (3, xr, o), (4, xf, c), (5, xf, o), (6, x, o)]
    for i, xx, cc in spots:
        got(ssq.at[xx * 2 + cc], ssnd.at[i], srcv.at[i])
    total = ssq[0]
    for i in range(1, 8):
        total = total + ssq[i]
    factor = lax.rsqrt(total * (1.0 / 1024.0) + EPS)
    fcol[...] = jnp.concatenate([factor, jnp.zeros((120, 128), F32)], axis=0).T

    lane = lax.broadcasted_iota(jnp.int32, (128, 128), 1)

    def pick(k):
        return jnp.sum(jnp.where(lane == k, fcol[...], 0.0), axis=1, keepdims=True)

    def partial(t, hs):
        rows = pl.ds(pl.multiple_of(t * 128, 128), 128)
        both = jnp.concatenate([ax[0, rows], ax[1, rows]], axis=1)
        fa, fp = pick(t), pick(t + 4)
        for h in hs:
            term = dot(both, w2[0, :, h * 512 : (h + 1) * 512])
            part[t, h] = (term * fa + bpart[t, h] * fp).astype(BF)

    def rrows(cc):
        return pl.ds(pl.multiple_of(cc * ROWS, ROWS), ROWS)

    partial(xf, (0, 1))
    send(part.at[xf, 0], far.at[0], rsnd.at[0], rrcv.at[0], at(z, xr, c))
    send(part.at[xf, 1], far.at[1], rsnd.at[1], rrcv.at[1], at(z, xl, c))
    partial(xr, (1, 0))
    partial(xl, (0, 1))
    for cc in (0, 1):
        send(part.at[xr, 1, rrows(cc)], fin.at[c, 2], esnd.at[2, cc], ercv.at[c, 2], at(z, xr, cc))
        send(part.at[xl, 0, rrows(cc)], fin.at[c, 0], esnd.at[0, cc], ercv.at[c, 0], at(z, xl, cc))
    partial(x, (0, 1))
    send(part.at[x, :, rrows(o)], ownp, rsnd.at[2], rrcv.at[2], at(z, x, o))
    got(far.at[0], rsnd.at[0], rrcv.at[0])
    part[xr, 0] = (part[xr, 0].astype(F32) + far[0].astype(F32)).astype(BF)
    for cc in (0, 1):
        send(part.at[xr, 0, rrows(cc)], fin.at[c, 1], esnd.at[1, cc], ercv.at[c, 1], at(z, xr, cc))
    got(far.at[1], rsnd.at[1], rrcv.at[1])
    part[xl, 1] = (part[xl, 1].astype(F32) + far[1].astype(F32)).astype(BF)
    for cc in (0, 1):
        send(part.at[xl, 1, rrows(cc)], fin.at[c, 3], esnd.at[3, cc], ercv.at[c, 3], at(z, xl, cc))

    got(ownp, rsnd.at[2], rrcv.at[2])
    for h in (0, 1):
        for i in range(4):
            got(fin.at[h, i], esnd.at[i, h], ercv.at[h, i])
    for h in (0, 1):
        for sub in (0, 1):
            mixed = fin[h, 2 * sub].astype(F32) + fin[h, 2 * sub + 1].astype(F32)
            here = jnp.where(c == h, part[x, sub, rrows(c)].astype(F32), ownp[sub].astype(F32))
            lo = h * 1024 + sub * 512
            out[0, :, lo : lo + 512] = (mixed + here).astype(BF)

    for i in range(3):
        sent(own, gsnd.at[i], grcv.at[i])
        sent(trows(x, 0), tsnd.at[0, i], trcv.at[0, i])
        sent(trows(x, 0), tsnd.at[1, i], trcv.at[1, i])
    for i in range(4):
        sent(nt.at[p], vsnd.at[i], vrcv.at[i])
        sent(own, osnd.at[15, i], orcv.at[15, i])
    for i in (0, 1):
        sent(w2.at[i, wrows], wsnd.at[i], wrcv.at[i])
        sent(px.at[c], psnd.at[i], prcv.at[i])
        sent(far.at[i], rsnd.at[i], rrcv.at[i])
    sent(rim, hsnd.at[0], hrcv.at[0])
    sent(ownp, rsnd.at[2], rrcv.at[2])
    for i in range(7):
        sent(ssq.at[p], ssnd.at[i], srcv.at[i])
    for i in range(4):
        for cc in (0, 1):
            sent(fin.at[0, i], esnd.at[i, cc], ercv.at[0, i])

    def drain(s, carry):
        for k in range(3):
            sent(own, usnd.at[s, k], urcv.at[s, k])
        sent(own, ysnd.at[0, s], yrcv.at[0, s])
        for r in range(4):
            sent(own, osnd.at[2 * s, r], orcv.at[2 * s, r])

        @pl.when(s < 7)
        def _():
            for k in range(3):
                sent(own, dsnd.at[s, k], drcv.at[s, k])
            sent(own, ysnd.at[1, s], yrcv.at[1, s])
            for r in range(4):
                sent(own, osnd.at[2 * s + 1, r], orcv.at[2 * s + 1, r])

        return carry

    lax.fori_loop(0, 8, drain, 0)


def rope_table(length):
    halfway = 16
    inv = (1.0 / np.float32(THETA) ** (np.arange(halfway, dtype=np.float32) / np.float32(halfway))).astype(np.float32)
    angle = (np.arange(length, dtype=np.float32)[None, :] * inv[:, None]).astype(np.float32).astype(np.float64)
    return np.concatenate([np.cos(angle), np.sin(angle)], axis=0).astype(np.float32)


def local(
    tokens, input_gain, query_weight, latent_down, rotary_down, pool_down, key_up, value_up,
    query_gain, key_gain, pool_weight, pool_scale, attention_gain, pool_gain, attention_out, pool_out,
):
    width = tokens.shape[2]
    table = jnp.asarray(rope_table(NS * BLOCK))
    hbm = pl.BlockSpec(memory_space=pl.ANY)
    vmem = pl.BlockSpec(memory_space=pltpu.VMEM)
    V = pltpu.VMEM
    D = pltpu.SemaphoreType.DMA
    half = width // 2
    scratch = [
        V((ROWS, width), BF), V((8, ROWS, width), BF), V((width, QK), BF), V((width, 256), BF),
        V((width, 32), BF), V((width, 128), BF), V((256, 128), BF), V((256, 128), BF),
        V((2, 64, 64), BF), V((2, 256, half), BF), V((32, NS * BLOCK), F32),
        V((NS, 2, NX, 144, 128), BF), V((128, 256), BF), V((128, 256), BF), V((BLOCK, 128), BF),
        V((128, BLOCK), BF), V((256, BLOCK), BF), V((BLOCK, 256), F32), V((QK, 128), F32), V((QK, 128), F32),
        V((RIM, 128), BF), V((RIM, 128), BF), V((BLOCK + RIM, 128), F32), V((2, BLOCK, 128), BF),
        V((2, BLOCK, 128), BF), V((NX, 2, 128, half // 2), F32),
        V((8, 8, 128), F32), V((NX, 2, 128, half // 2), BF), V((2, 128, half // 2), BF),
        V((2, 4, ROWS, half // 2), BF), V((2, ROWS, half // 2), BF), V((128, 128), F32),
        D((11,)),
        D((8, 3)), D((8, 3)), D((7, 3)), D((7, 3)), D((2, 8)), D((2, 8)), D((3,)), D((3,)),
        D((16, 4)), D((16, 4)), D((2,)), D((2,)),
        D((2, 3)), D((2, 3)), D((4,)), D((4,)), D((2,)), D((2,)), D((1,)), D((1,)),
        D((4, 2)), D((2, 4)), D((7,)), D((7,)), D((3,)), D((3,)),
    ]
    args = (
        tokens, input_gain.reshape(1, -1), query_weight, latent_down, rotary_down, pool_down, key_up, value_up,
        query_gain.reshape(1, -1), key_gain.reshape(1, -1), pool_weight, pool_scale.reshape(1, -1),
        attention_gain.reshape(1, -1), pool_gain.reshape(1, -1), attention_out, pool_out, table,
    )
    specs = [hbm, vmem, hbm, hbm, hbm, hbm, hbm, hbm, vmem, vmem, hbm, vmem, vmem, vmem, hbm, hbm, hbm]
    return pl.pallas_call(
        kernel,
        out_shape=jax.ShapeDtypeStruct(tokens.shape, BF),
        in_specs=specs,
        out_specs=vmem,
        scratch_shapes=scratch,
        compiler_params=pltpu.CompilerParams(
            collective_id=0, has_side_effects=True, vmem_limit_bytes=60 * 1024 * 1024
        ),
    )(*args)


def solution(mesh):
    placed = (
        P("fs", ("sp", "tp"), None), P(), P(None, "tp"), P(), P(), P(None, "tp"), P(), P(),
        P(), P(), P(), P("tp"), P("tp"), P("tp"), P("tp", None), P("tp", None),
    )
    return jax.shard_map(
        local, mesh=mesh, in_specs=placed, out_specs=P("fs", ("sp", "tp"), None), check_vma=False
    )
```

```python
import functools
import math

import jax
import jax.numpy as jnp
import numpy as np
from jax import lax
from jax.experimental import pallas as pl
from jax.experimental.pallas import tpu as pltpu
from jax.sharding import PartitionSpec as P

MESH = pl.DeviceIdType.MESH
BF = jnp.bfloat16
F32 = jnp.float32

EPS = 1e-06
THETA = 10000.0
QK = 96
SCALE = math.log2(math.e) / math.sqrt(QK)
NX = 4
NS = 16
BLOCK = 512
ROWS = 64
RIM = 16
START = 13


def dot(a, b, dims=((1,), (0,)), precision=None):
    return lax.dot_general(a, b, (dims, ((), ())), preferred_element_type=F32, precision=precision)


def kernel(
    tokens, igh, qw, ld, rd, pd, ku, vu, qgh, kgh, pw, psh, agh, pgh, ao, po, tab,
    out,
    tokv, ig, nt, qwv, ldv, rdv, wv, kuv, vuv, qg, kg, pwv, ps, ag, pg, w2, tabv,
    xt, kut, vut, qv, ktv, vtv, acc, qcol, kcol, rim, halo, poolin, px, ax, bpart,
    ssq, part, far, fin, ownp, fcol,
    dsem, usnd, urcv, dsnd, drcv, ysnd, yrcv, gsnd, grcv, osnd, orcv, nsnd, psnd, prcv,
    tsnd, trcv, vsnd, vrcv, wsnd, wrcv, hsnd, hrcv, esnd, ercv, ssnd, srcv, rsnd, rrcv,
):
    z = lax.axis_index("sp")
    fs = lax.axis_index("fs")
    p = lax.axis_index("tp")
    c = lax.rem(p, 2)
    x = p // 2
    o = 1 - c

    def zmod(v):
        return lax.rem(v + 2 * NS, NS)

    def xmod(v):
        return lax.rem(v + 2 * NX, NX)

    def at(zz, xx, cc):
        return (zz, fs, xx * 2 + cc)

    xr, xl, xf = xmod(x + 1), xmod(x - 1), xmod(x + 2)
    zu, zd = zmod(z + 1), zmod(z - 1)

    def send(src, dst, ssem, rsem, dev):
        copy = pltpu.make_async_remote_copy(
            src_ref=src, dst_ref=dst, send_sem=ssem, recv_sem=rsem, device_id=dev, device_id_type=MESH
        )
        copy.start()

    def got(dst, ssem, rsem):
        pltpu.make_async_remote_copy(
            src_ref=dst, dst_ref=dst, send_sem=ssem, recv_sem=rsem,
            device_id=at(z, x, o), device_id_type=MESH,
        ).wait_recv()

    def sent(src, ssem, rsem):
        pltpu.make_async_remote_copy(
            src_ref=src, dst_ref=src, send_sem=ssem, recv_sem=rsem,
            device_id=at(z, x, o), device_id_type=MESH,
        ).wait_send()

    half = out.shape[2] // 2
    mine = pl.ds(pl.multiple_of(c * half, 128), half)
    theirs = pl.ds(pl.multiple_of(o * half, 128), half)
    kcols = pl.ds(pl.multiple_of(x * 128, 128), 128)
    vcols = pl.ds(pl.multiple_of(p * 128, 128), 128)
    wrows = pl.ds(pl.multiple_of(c * 128, 128), 128)
    loads = [
        (tokens.at[0], tokv),
        (ld, ldv),
        (rd, rdv),
        (qw, qwv),
        (pd, wv.at[:, 0:128]),
        (ku.at[:, kcols], kuv),
        (vu.at[:, vcols], vuv),
        (pw.at[pl.ds(p * 2, 2)], pwv),
        (tab, tabv),
        (ao.at[:, mine], w2.at[0, wrows]),
        (po.at[:, mine], w2.at[1, wrows]),
        (igh, ig),
        (qgh, qg),
        (kgh, kg),
        (psh, ps),
        (agh, ag),
        (pgh, pg),
    ]
    copies = [pltpu.make_async_copy(s, d, dsem.at[i]) for i, (s, d) in enumerate(loads)]
    for i in (0, 11, 1, 2, 5, 6, 12, 13, 3, 4, 8, 7, 9, 10, 14, 15, 16):
        copies[i].start()

    barrier = pltpu.get_barrier_semaphore()
    peers = [at(z, x, o), at(zu, x, c), at(zd, x, c)]
    peers += [at(z, xx, cc) for xx in (xr, xl, xf) for cc in (c, o)]
    for peer in peers:
        pl.semaphore_signal(barrier, inc=1, device_id=peer, device_id_type=MESH)

    copies[0].wait()
    copies[11].wait()
    source = tokv[...].astype(F32)
    scale = lax.rsqrt(jnp.mean(source * source, axis=1, keepdims=True) + EPS)
    normed = (source * scale * ig[...]).astype(BF)
    nt[p] = normed
    copies[1].wait()
    copies[2].wait()
    latent = dot(normed, ldv[...]).astype(BF).astype(F32)
    rotary = dot(rdv[...], normed, ((1,), (1,))).astype(BF).astype(F32)
    swap = (lax.broadcasted_iota(jnp.int32, (16, ROWS), 0) + c * 16) >= 16
    turned = [jnp.where(swap, rotary[16:32], rotary[:16]), jnp.where(swap, rotary[:16], rotary[16:32])]
    lat = latent * lax.rsqrt(jnp.mean(latent * latent, axis=1, keepdims=True) + EPS)
    swap = (lax.broadcasted_iota(jnp.int32, (ROWS, 128), 0) + c * 2 * ROWS) >= 2 * ROWS
    stacked = jnp.concatenate(
        [jnp.where(swap, lat[:, 128:], lat[:, :128]), jnp.where(swap, lat[:, :128], lat[:, 128:])], axis=0
    )
    xt[z, x, c, 0:128, :] = stacked.T.astype(BF)
    xt[z, x, c, 128:144, :] = jnp.concatenate(turned, axis=1).astype(BF)

    pl.semaphore_wait(barrier, len(peers))

    rows_core, ring_core = c == 0, c == 1
    own = xt.at[z, x]
    piece = xt.at[z, x, c]

    def up(s, k, pair):
        send(pair, pair, usnd.at[lax.rem(s, 2)], urcv.at[s, k], at(zu, x, 1))

    def down(s, k, pair):
        send(pair, pair, dsnd.at[lax.rem(s, 2)], drcv.at[s, k], at(zd, x, 1))

    def other(ssem, sem, j):
        send(xt.at[j], xt.at[j], ssem, orcv.at[sem], at(z, x, 0))

    def goes_up(s):
        return (z - s >= 0) & (z < NS - 1)

    def goes_down(s):
        return (z + s <= 6) | (z + s >= NS)

    @pl.when(rows_core)
    def _():
        send(piece, piece, gsnd.at[0], grcv.at[0, 0], at(z, x, 1))

    send(piece, piece, gsnd.at[0], grcv.at[3, c], at(z, xr, 1))
    send(piece, piece, gsnd.at[0], grcv.at[1, c], at(z, xl, 1))
    send(piece, piece, gsnd.at[0], grcv.at[2, c], at(z, xf, 1))

    def trows(xx, h):
        return nt.at[xx * 2 + h]

    def right(h, i, xx):
        send(trows(xx, h), trows(xx, h), tsnd.at[0], trcv.at[0, i], at(z, xr, 0))

    def left(h, i, xx):
        send(trows(xx, h), trows(xx, h), tsnd.at[0], trcv.at[1, i], at(z, xl, 0))

    send(nt.at[p], nt.at[p], vsnd.at[0], vrcv.at[0], at(z, x, o))

    @pl.when(rows_core)
    def _():
        right(0, 0, x)
        got(trows(x, 1), vsnd.at[0], vrcv.at[0])
        left(1, 1, x)
        right(1, 1, x)
        left(0, 0, x)

    @pl.when(ring_core)
    def _():
        got(piece, gsnd.at[0], grcv.at[0, 0])

        @pl.when(goes_up(0))
        def _():
            up(0, 0, own)

        @pl.when(goes_down(0))
        def _():
            down(0, 0, own)

    for i, w in enumerate((ao, po)):
        send(w.at[:, theirs], w2.at[i, wrows], wsnd.at[0], wrcv.at[0], at(z, x, o))

    copies[5].wait()
    copies[6].wait()
    kut[...] = kuv[...].astype(F32).T.astype(BF)
    vut[...] = vuv[...].astype(F32).T.astype(BF)
    copies[12].wait()
    copies[13].wait()
    qcol[...] = jnp.broadcast_to(qg[...], (128, QK)).T
    kcol[...] = jnp.broadcast_to(kg[...], (128, QK)).T
    acc[...] = jnp.zeros_like(acc)
    copies[3].wait()
    for i in range(qwv.shape[1] // 128):
        cols = slice(i * 128, (i + 1) * 128)
        tile = jnp.concatenate([qwv[:, cols].astype(F32), jnp.zeros((128 - QK, 128), F32)], axis=0)
        wv[cols, 128:256] = tile.T.astype(BF)

    def gathered(rel):
        pair = xt.at[z, xmod(x + rel)]
        for i in (0, 1):
            got(piece, gsnd.at[0], grcv.at[rel, i])
        if rel != 1:

            @pl.when(goes_up(0))
            def _():
                up(0, 4 - rel, pair)

        if rel != 3:

            @pl.when(goes_down(0))
            def _():
                down(0, rel, pair)

    @pl.when(ring_core)
    def _():
        gathered(1)
        gathered(3)

    copies[8].wait()

    def rotate(a, b, first):
        cosine = tabv[0:16, pl.ds(first, a.shape[1])]
        sine = tabv[16:32, pl.ds(first, a.shape[1])]
        return a * cosine - b * sine, b * cosine + a * sine

    def expand(j):
        lane = lax.broadcasted_iota(jnp.int32, (144, 128), 1)
        low, high = [], []
        for xx in range(NX):
            p0 = xt[j, xx, 0].astype(F32)
            p1 = xt[j, xx, 1].astype(F32)
            low.append(jnp.where(lane < 64, p0, p1))
            high.append(pltpu.roll(jnp.where(lane < 64, p1, p0), 64, 1))
        low = jnp.concatenate(low, axis=1)
        high = jnp.concatenate(high, axis=1)
        lat2 = jnp.concatenate([low[:128].astype(BF), high[:128].astype(BF)], axis=0)
        plain = dot(kut[pl.ds(pl.multiple_of(c * 64, 64), 64), :], lat2)
        vtv[j] = dot(vut[...], lat2).astype(BF)
        a, b = low[128:144], high[128:144]
        total = jnp.sum(plain * plain, axis=0, keepdims=True)
        total = total + jnp.sum(a * a + b * b, axis=0, keepdims=True)
        factor = lax.rsqrt(total * (1.0 / QK) + EPS)
        gain = kcol[:, 0:1]
        first = pl.multiple_of(j * BLOCK, 128)
        a, b = rotate(a * factor * gain[64:80], b * factor * gain[80:96], first)
        ktv[j, 0:64, :] = (plain * factor * gain[0:64]).astype(BF)
        ktv[j, 64:80, :] = a.astype(BF)
        ktv[j, 80:96, :] = b.astype(BF)
        ktv[j, QK:128, :] = jnp.zeros((128 - QK, BLOCK), BF)

    def attend(j, masked):
        both = jnp.concatenate([vtv[j], jnp.ones((128, BLOCK), BF)], axis=0)
        weight = jnp.exp2(dot(qv[...], ktv[j]))
        if masked:
            qpos = lax.broadcasted_iota(jnp.int32, weight.shape, 0)
            kpos = lax.broadcasted_iota(jnp.int32, weight.shape, 1)
            weight = jnp.where(kpos <= qpos, weight, 0.0)
        acc[...] += dot(weight.astype(BF), both, ((1,), (1,)))

    def block_of(u):
        return jnp.where(lax.rem(u, 2) == 1, z - (u + 1) // 2, z + u // 2 - NS)

    def unit(u, carry):
        j = block_of(u)

        @pl.when(j >= 0)
        def _():
            attend(j, False)

        return carry

    def project(chips):
        rows = [nt[2 * t + i] for t in chips for i in (0, 1)]
        both = dot(jnp.concatenate(rows, axis=0), wv[...])
        raws = both[:, 128:].T[:QK]
        for i, t in enumerate(chips):
            spot = pl.ds(pl.multiple_of(t * 128, 128), 128)
            poolin[pl.ds(pl.multiple_of(t * 128 + RIM, 8), 128), :] = (
                both[i * 128 : (i + 1) * 128, :128].astype(BF).astype(F32)
            )
            raw = raws[:, i * 128 : (i + 1) * 128]
            total = jnp.sum(raw * raw, axis=0, keepdims=True)
            normal = raw * lax.rsqrt(total * (1.0 / QK) + EPS) * qcol[:, 0:1] * SCALE
            first = pl.multiple_of(z * BLOCK + t * 128, 128)
            a, b = rotate(normal[64:80], normal[80:96], first)
            full = jnp.concatenate([normal[:64], a, b, jnp.zeros((32, 128), F32)], axis=0)
            qv[spot, :] = full.T.astype(BF)

    def sumsq(values):
        return dot(jnp.ones((8, 128), F32), values * values, ((1,), (1,)), lax.Precision.HIGHEST)

    def spread(totals, start):
        sub = lax.broadcasted_iota(jnp.int32, (8, 128), 0)
        packed = jnp.zeros((8, 128), F32)
        for t in range(NX):
            packed = jnp.where(sub == start + t, totals[:, t * 128 : (t + 1) * 128], packed)
        return packed

    def pool():
        @pl.when(z > 0)
        def _():
            got(halo, hsnd.at[0], hrcv.at[0])

        poolin[0:RIM, :] = jnp.where(z > 0, halo[...].astype(F32), 0.0)
        values = poolin[...]
        two = values + pltpu.roll(values, 1, 0)
        four = two + pltpu.roll(two, 2, 0)
        eight = four + pltpu.roll(four, 4, 0)
        sixteen = eight + pltpu.roll(eight, 8, 0)
        lane = lax.broadcasted_iota(jnp.int32, (BLOCK, 128), 1)
        wide = c == 1
        left = jnp.where(wide ^ (x < 0), eight, two)[RIM:]
        right = jnp.where(wide ^ (x < 0), sixteen, four)[RIM:]
        total = jnp.where(lane < 64, left, right)
        base = jnp.where(wide, 8.0, 2.0)
        window = jnp.where(lane < 64, base, base * 2.0)
        count = (lax.broadcasted_iota(jnp.int32, (BLOCK, 128), 0) + (z * BLOCK + 1)).astype(F32)
        mean = (total / jnp.minimum(count, window) - values[RIM:]).astype(BF)
        zero = jnp.zeros((64, 64), F32)
        w0 = jnp.concatenate([pwv[0].astype(F32), zero], axis=1)
        w1 = jnp.concatenate([zero, pwv[1].astype(F32)], axis=1)
        copies[14].wait()
        copies[16].wait()
        pooled = dot(mean, jnp.concatenate([w0, w1], axis=0).astype(BF)) * ps[...]
        ssq[p] = spread(sumsq(pooled), 4)
        px[c] = (pooled * pg[...]).astype(BF)
        send(px.at[c], px.at[c], psnd.at[0], prcv.at[0], at(z, x, o))

    def project_pool():
        got(px.at[o], psnd.at[0], prcv.at[0])
        for i in (0, 1):
            copies[9 + i].wait()
        got(w2.at[:, pl.ds(pl.multiple_of(o * 128, 128), 128)], wsnd.at[0], wrcv.at[0])

        def chunk(t, carry):
            rows = pl.ds(pl.multiple_of(t * 128, 128), 128)
            both = jnp.concatenate([px[0, rows], px[1, rows]], axis=1)
            for h in (0, 1):
                bpart[t, h] = dot(both, w2[1, :, h * 512 : (h + 1) * 512])
            return carry

        lax.fori_loop(0, NX, chunk, 0)

    own_block = xt.at[z]

    def piece_up(s, k):
        return xt.at[zmod(z - s), xmod(x - k)]

    def piece_down(s, k):
        return xt.at[zmod(z + s), xmod(x + k)]

    def from_below(s):
        return z - s >= 0

    def from_above(s):
        return z + s >= NS

    def slot(n, carry):
        s, k = n // 3 + 1, lax.rem(n, 3)

        @pl.when(ring_core & from_below(s) & (s < 9))
        def _():
            pair = piece_up(s, k)
            got(pair, usnd.at[0], urcv.at[s - 1, k])

            @pl.when((k == 0) & (s >= 2) & goes_up(s - 2) & (s < 8))
            def _():
                sent(xt.at[z, 0:3], usnd.at[lax.rem(s, 2)], urcv.at[0, 0])

            @pl.when((s < 8) & (z < NS - 1))
            def _():
                up(s, k, pair)

            @pl.when(k == 0)
            def _():
                @pl.when(s >= 3)
                def _():
                    sent(own, ysnd.at[0, lax.rem(s, 2)], yrcv.at[0, 0])

                send(pair, pair, ysnd.at[0, lax.rem(s, 2)], yrcv.at[0, s - 1], at(z, xl, 1))

        @pl.when(ring_core & goes_down(s) & (s < 8))
        def _():
            pair = piece_down(s, k)
            got(pair, dsnd.at[0], drcv.at[s - 1, k])

            @pl.when(s < 7)
            def _():
                @pl.when((k == 0) & (s >= 2) & goes_down(s - 2))
                def _():
                    sent(xt.at[z, 0:3], dsnd.at[lax.rem(s, 2)], drcv.at[0, 0])

                down(s, k, pair)

            @pl.when((k == 0) & from_above(s))
            def _():
                @pl.when((s >= 3) & from_above(s - 2))
                def _():
                    sent(own, ysnd.at[1, lax.rem(s, 2)], yrcv.at[1, 0])

                send(pair, pair, ysnd.at[1, lax.rem(s, 2)], yrcv.at[1, s - 1], at(z, xr, 1))

        @pl.when(ring_core & (n == 0))
        def _():
            gathered(2)
            send(piece, piece, nsnd.at[0], orcv.at[15], at(z, x, 0))
            for i, xx in enumerate((xr, xl, xf)):
                pair = xt.at[z, xx]
                send(pair, pair, nsnd.at[0], orcv.at[16 + i], at(z, x, 0))

        @pl.when(ring_core & (n == 6))
        def _():
            sides(1)

        @pl.when(ring_core & (k == 0) & (s >= 3))
        def _():
            sides(s - 1)

        @pl.when(rows_core & (n == 0))
        def _():
            got(trows(xl, 0), tsnd.at[0], trcv.at[0, 0])
            right(0, 2, xl)
            got(trows(xr, 1), tsnd.at[0], trcv.at[1, 1])
            left(1, 2, xr)

        @pl.when(n == 3)
        def _():
            @pl.when(rows_core)
            def _():
                got(xt.at[z, x, 1], nsnd.at[0], orcv.at[15])
                for i, xx in enumerate((xr, xl, xf)):
                    got(xt.at[z, xx], nsnd.at[0], orcv.at[16 + i])

            expand(z)

        def pass_on(i, xx):
            block = nt.at[pl.ds(xx * 2, 2)]
            send(block, block, vsnd.at[0], vrcv.at[i], at(z, x, 1))

        def passed(i, xx):
            got(nt.at[pl.ds(xx * 2, 2)], vsnd.at[0], vrcv.at[i])

        @pl.when(rows_core & (n == 5))
        def _():
            got(trows(xl, 1), tsnd.at[0], trcv.at[0, 1])
            pass_on(1, xl)
            got(trows(xr, 0), tsnd.at[0], trcv.at[1, 0])
            pass_on(2, xr)

        @pl.when(n == 8)
        def _():
            copies[4].wait()

            @pl.when(ring_core)
            def _():
                got(trows(x, 0), vsnd.at[0], vrcv.at[0])
                passed(1, xl)
                passed(2, xr)

            project((x, xl, xr))

        @pl.when(rows_core & (n == 10))
        def _():
            got(trows(xf, 0), tsnd.at[0], trcv.at[0, 2])
            got(trows(xf, 1), tsnd.at[0], trcv.at[1, 2])
            pass_on(3, xf)

        @pl.when(n == 12)
        def _():
            @pl.when(ring_core)
            def _():
                passed(3, xf)

            project((xf,))
            rim[...] = poolin[BLOCK:, :].astype(BF)

            @pl.when(z < NS - 1)
            def _():
                send(rim, halo, hsnd.at[0], hrcv.at[0], at(zu, x, c))

        @pl.when(n == START)
        def _():
            attend(z, True)

        @pl.when(n == START + 2)
        def _():
            copies[7].wait()
            pool()

        @pl.when(n == START + 5)
        def _():
            project_pool()

        e = jnp.where(k == 2, 2 * s - 3, 2 * s - 4)
        e = jnp.where(n == 10, 1, jnp.where(n == 13, 2, e))
        due = ((k == 2) & (s >= 3)) | ((k == 0) & (s >= 4)) | (n == 10) | (n == 13)
        je = block_of(e)
        due = due & (je >= 0)
        lo, hi = limit(n - 1) + 1, limit(n)
        ja = block_of(lo)
        ripe = (lo <= hi) & (ja >= 0)

        @pl.when(due & rows_core)
        def _():
            got(xt.at[je], nsnd.at[0], orcv.at[e - 1])

        @pl.when(due & ripe)
        def _():
            attend(ja, False)
            expand(je)

        @pl.when(due & jnp.logical_not(ripe))
        def _():
            expand(je)

        @pl.when(ripe & jnp.logical_not(due))
        def _():
            attend(ja, False)

        lax.fori_loop(lo + 1, hi + 1, unit, 0)
        return carry

    def limit(n):
        ready = jnp.maximum(2 * (n // 3) - 3, 2 * ((n - 1) // 3) - 2)
        return jnp.maximum(jnp.minimum(ready, (5 * (n - START) + 3) // 4), 0)

    def sides(s):
        @pl.when(from_below(s))
        def _():
            pair = xt.at[zmod(z - s), xr]
            got(pair, ysnd.at[0, 0], yrcv.at[0, s - 1])
            ssem = osnd.at[0, lax.rem(s, 2)]

            @pl.when(s >= 3)
            def _():
                sent(own_block, ssem, orcv.at[15])

            other(ssem, 2 * s - 2, zmod(z - s))

        @pl.when(from_above(s) & (s < 8))
        def _():
            pair = xt.at[zmod(z + s), xl]
            got(pair, ysnd.at[1, 0], yrcv.at[1, s - 1])
            ssem = osnd.at[1, lax.rem(s, 2)]

            @pl.when((s >= 3) & from_above(s - 2))
            def _():
                sent(own_block, ssem, orcv.at[15])

            other(ssem, 2 * s - 1, zmod(z + s))

    lax.fori_loop(0, 27, slot, 0)
    lax.fori_loop(limit(26) + 1, 16, unit, 0)

    copies[15].wait()
    attended = acc[:, :128] / acc[:, 128:]
    ssq[p] = ssq[p] + spread(sumsq(attended), 0)
    ax[c] = (attended * ag[...]).astype(BF)
    send(ax.at[c], ax.at[c], psnd.at[1], prcv.at[1], at(z, x, o))
    tpeers = [(0, xr, c), (1, xr, o), (2, xl, c), (3, xl, o), (4, xf, c), (5, xf, o), (6, x, o)]
    for i, xx, cc in tpeers:
        send(ssq.at[p], ssq.at[p], ssnd.at[0], srcv.at[0], at(z, xx, cc))
    got(ax.at[o], psnd.at[1], prcv.at[1])
    got(ssq.at[0:7], ssnd.at[0], srcv.at[0])
    total = ssq[0]
    for i in range(1, 8):
        total = total + ssq[i]
    factor = lax.rsqrt(total * (1.0 / 1024.0) + EPS)
    fcol[...] = jnp.concatenate([factor, jnp.zeros((120, 128), F32)], axis=0).T

    lane = lax.broadcasted_iota(jnp.int32, (128, 128), 1)

    def pick(k):
        return jnp.sum(jnp.where(lane == k, fcol[...], 0.0), axis=1, keepdims=True)

    def partial(t, hs):
        rows = pl.ds(pl.multiple_of(t * 128, 128), 128)
        both = jnp.concatenate([ax[0, rows], ax[1, rows]], axis=1)
        fa, fp = pick(t), pick(t + 4)
        for h in hs:
            term = dot(both, w2[0, :, h * 512 : (h + 1) * 512])
            part[t, h] = (term * fa + bpart[t, h] * fp).astype(BF)

    def rrows(cc):
        return pl.ds(pl.multiple_of(cc * ROWS, ROWS), ROWS)

    partial(xf, (0, 1))
    send(part.at[xf, 0], far.at[0], rsnd.at[0], rrcv.at[0], at(z, xr, c))
    send(part.at[xf, 1], far.at[1], rsnd.at[0], rrcv.at[1], at(z, xl, c))
    partial(xr, (1, 0))
    partial(xl, (0, 1))
    for cc in (0, 1):
        send(part.at[xr, 1, rrows(cc)], fin.at[c, 2], esnd.at[0], ercv.at[0], at(z, xr, cc))
        send(part.at[xl, 0, rrows(cc)], fin.at[c, 0], esnd.at[0], ercv.at[0], at(z, xl, cc))
    partial(x, (0, 1))
    send(part.at[x, :, rrows(o)], ownp, rsnd.at[1], rrcv.at[2], at(z, x, o))
    got(far.at[0], rsnd.at[0], rrcv.at[0])
    part[xr, 0] = (part[xr, 0].astype(F32) + far[0].astype(F32)).astype(BF)
    for cc in (0, 1):
        send(part.at[xr, 0, rrows(cc)], fin.at[c, 1], esnd.at[0], ercv.at[0], at(z, xr, cc))
    got(far.at[1], rsnd.at[0], rrcv.at[1])
    part[xl, 1] = (part[xl, 1].astype(F32) + far[1].astype(F32)).astype(BF)
    for cc in (0, 1):
        send(part.at[xl, 1, rrows(cc)], fin.at[c, 3], esnd.at[0], ercv.at[0], at(z, xl, cc))

    got(ownp, rsnd.at[1], rrcv.at[2])
    got(fin, esnd.at[0], ercv.at[0])
    for h in (0, 1):
        for sub in (0, 1):
            mixed = fin[h, 2 * sub].astype(F32) + fin[h, 2 * sub + 1].astype(F32)
            here = jnp.where(c == h, part[x, sub, rrows(c)].astype(F32), ownp[sub].astype(F32))
            lo = h * 1024 + sub * 512
            out[0, :, lo : lo + 512] = (mixed + here).astype(BF)

    @pl.when(rows_core)
    def _():
        sent(xt.at[z, 0:2], gsnd.at[0], grcv.at[0, 0])
        sent(nt.at[0:6], tsnd.at[0], trcv.at[0, 0])
        sent(nt.at[0:7], vsnd.at[0], vrcv.at[0])

    @pl.when(ring_core)
    def _():
        sent(xt.at[z, 0:3, 0], gsnd.at[0], grcv.at[0, 0])
        sent(nt.at[p], vsnd.at[0], vrcv.at[0])
        sent(xt.at[0:7, 0, 0], nsnd.at[0], orcv.at[15])

    sent(w2.at[:, wrows], wsnd.at[0], wrcv.at[0])
    for i in (0, 1):
        sent(px.at[c], psnd.at[i], prcv.at[i])
    sent(far, rsnd.at[0], rrcv.at[0])
    sent(ownp, rsnd.at[1], rrcv.at[2])
    sent(ssq.at[0:7], ssnd.at[0], srcv.at[0])
    sent(fin, esnd.at[0], ercv.at[0])

    @pl.when(z < NS - 1)
    def _():
        sent(rim, hsnd.at[0], hrcv.at[0])

    def drain(s, carry):
        odd = lax.rem(s, 2)
        other_odd = 1 - odd

        @pl.when(goes_up(s) & jnp.logical_not(goes_up(s + 2) & (s < 6)))
        def _():
            sent(xt.at[z, 0:3], usnd.at[odd], urcv.at[0, 0])

        @pl.when(goes_down(s) & (s < 7) & jnp.logical_not(goes_down(s + 2) & (s < 5)))
        def _():
            sent(xt.at[z, 0:3], dsnd.at[odd], drcv.at[0, 0])

        @pl.when(from_below(s + 1) & jnp.logical_not(from_below(s + 3) & (s < 6)))
        def _():
            sent(own, ysnd.at[0, other_odd], yrcv.at[0, 0])
            sent(own_block, osnd.at[0, other_odd], orcv.at[15])

        @pl.when(from_above(s + 1) & (s < 7) & jnp.logical_not(from_above(s + 3) & (s < 5)))
        def _():
            sent(own, ysnd.at[1, other_odd], yrcv.at[1, 0])
            sent(own_block, osnd.at[1, other_odd], orcv.at[15])

        return carry

    @pl.when(ring_core)
    def _():
        lax.fori_loop(0, 8, drain, 0)


def rope_table(length):
    halfway = 16
    inv = (1.0 / np.float32(THETA) ** (np.arange(halfway, dtype=np.float32) / np.float32(halfway))).astype(np.float32)
    angle = (np.arange(length, dtype=np.float32)[None, :] * inv[:, None]).astype(np.float32).astype(np.float64)
    return np.concatenate([np.cos(angle), np.sin(angle)], axis=0).astype(np.float32)


def local(
    tokens, input_gain, query_weight, latent_down, rotary_down, pool_down, key_up, value_up,
    query_gain, key_gain, pool_weight, pool_scale, attention_gain, pool_gain, attention_out, pool_out,
):
    width = tokens.shape[2]
    table = jnp.asarray(rope_table(NS * BLOCK))
    hbm = pl.BlockSpec(memory_space=pl.ANY)
    vmem = pl.BlockSpec(memory_space=pltpu.VMEM)
    V = pltpu.VMEM
    D = pltpu.SemaphoreType.DMA
    half = width // 2
    scratch = [
        V((ROWS, width), BF), V((1, width), F32), V((8, ROWS, width), BF), V((QK, width), BF),
        V((width, 256), BF), V((32, width), BF), V((width, 256), BF), V((256, 128), BF), V((256, 128), BF),
        V((1, QK), F32), V((1, QK), F32), V((2, 64, 64), BF), V((1, 128), F32), V((1, 128), F32),
        V((1, 128), F32), V((2, 256, half), BF), V((32, NS * BLOCK), F32),
        V((NS, NX, 2, 144, 128), BF), V((128, 256), BF), V((128, 256), BF), V((BLOCK, 128), BF),
        V((NS, 128, BLOCK), BF), V((NS, 128, BLOCK), BF), V((BLOCK, 256), F32),
        V((QK, 128), F32), V((QK, 128), F32),
        V((RIM, 128), BF), V((RIM, 128), BF), V((BLOCK + RIM, 128), F32), V((2, BLOCK, 128), BF),
        V((2, BLOCK, 128), BF), V((NX, 2, 128, half // 2), F32),
        V((8, 8, 128), F32), V((NX, 2, 128, half // 2), BF), V((2, 128, half // 2), BF),
        V((2, 4, ROWS, half // 2), BF), V((2, ROWS, half // 2), BF), V((128, 128), F32),
        D((17,)),
        D((2,)), D((8, 3)), D((2,)), D((7, 3)), D((2, 2)), D((2, 8)), D((1,)), D((4, 2)),
        D((2, 2)), D((19,)), D((1,)), D((2,)), D((2,)),
        D((1,)), D((2, 3)), D((1,)), D((4,)), D((1,)), D((1,)), D((1,)), D((1,)),
        D((1,)), D((1,)), D((1,)), D((1,)), D((2,)), D((3,)),
    ]
    args = (
        tokens, input_gain.reshape(1, -1), query_weight.T, latent_down, rotary_down.T, pool_down, key_up, value_up,
        query_gain.reshape(1, -1), key_gain.reshape(1, -1), pool_weight, pool_scale.reshape(1, -1),
        attention_gain.reshape(1, -1), pool_gain.reshape(1, -1), attention_out, pool_out, table,
    )
    specs = [hbm] * 17
    return pl.pallas_call(
        kernel,
        out_shape=pltpu.VMEM(tokens.shape, BF),
        in_specs=specs,
        out_specs=vmem,
        scratch_shapes=scratch,
        compiler_params=pltpu.CompilerParams(
            collective_id=0, has_side_effects=True, vmem_limit_bytes=60 * 1024 * 1024
        ),
    )(*args)


def solution(mesh):
    placed = (
        P("fs", ("sp", "tp"), None), P(), P(None, "tp"), P(), P(), P(None, "tp"), P(), P(),
        P(), P(), P(), P("tp"), P("tp"), P("tp"), P("tp", None), P("tp", None),
    )
    return jax.shard_map(
        local, mesh=mesh, in_specs=placed, out_specs=P("fs", ("sp", "tp"), None), check_vma=False
    )
```

```python
import functools
import math

import jax
import jax.numpy as jnp
import numpy as np
from jax import lax
from jax.experimental import pallas as pl
from jax.experimental.pallas import tpu as pltpu
from jax.sharding import PartitionSpec as P

MESH = pl.DeviceIdType.MESH
BF = jnp.bfloat16
F32 = jnp.float32

EPS = 1e-06
THETA = 10000.0
QK = 96
SCALE = math.log2(math.e) / math.sqrt(QK)
NX = 4
NS = 16
BLOCK = 512
ROWS = 64
RIM = 16
START = 10


def dot(a, b, dims=((1,), (0,)), precision=None):
    return lax.dot_general(a, b, (dims, ((), ())), preferred_element_type=F32, precision=precision)


def kernel(
    tokens, igh, qw, ld, rd, pd, ku, vu, qgh, kgh, pw, psh, agh, pgh, ao, po, tab,
    out,
    tokv, ig, nt, qwv, ldv, rdv, wv, kuv, vuv, qg, kg, pwv, ps, ag, pg, w2, tabv,
    xt, kut, vut, qv, ktv, vtv, acc, qcol, kcol, rim, halo, poolin, px, ax, bpart,
    ssq, part, far, fin, ownp, fcol, fpool, fgot,
    dsem, usnd, urcv, dsnd, drcv, ysnd, yrcv, gsnd, grcv, osnd, orcv, nsnd, psnd, prcv,
    tsnd, trcv, vsnd, vrcv, wsnd, wrcv, hsnd, hrcv, esnd, ercv, ssnd, srcv, rsnd, rrcv, fsnd, frcv,
):
    z = lax.axis_index("sp")
    fs = lax.axis_index("fs")
    p = lax.axis_index("tp")
    c = lax.rem(p, 2)
    x = p // 2
    o = 1 - c

    def zmod(v):
        return lax.rem(v + 2 * NS, NS)

    def xmod(v):
        return lax.rem(v + 2 * NX, NX)

    def at(zz, xx, cc):
        return (zz, fs, xx * 2 + cc)

    xr, xl, xf = xmod(x + 1), xmod(x - 1), xmod(x + 2)
    zu, zd = zmod(z + 1), zmod(z - 1)

    def send(src, dst, ssem, rsem, dev):
        copy = pltpu.make_async_remote_copy(
            src_ref=src, dst_ref=dst, send_sem=ssem, recv_sem=rsem, device_id=dev, device_id_type=MESH
        )
        copy.start()

    def got(dst, ssem, rsem):
        pltpu.make_async_remote_copy(
            src_ref=dst, dst_ref=dst, send_sem=ssem, recv_sem=rsem,
            device_id=at(z, x, o), device_id_type=MESH,
        ).wait_recv()

    def sent(src, ssem, rsem):
        pltpu.make_async_remote_copy(
            src_ref=src, dst_ref=src, send_sem=ssem, recv_sem=rsem,
            device_id=at(z, x, o), device_id_type=MESH,
        ).wait_send()

    barrier = pltpu.get_barrier_semaphore()
    peers = [at(z, x, o), at(zu, x, c), at(zd, x, c)]
    peers += [at(z, xx, cc) for xx in (xr, xl, xf) for cc in (c, o)]
    for peer in peers:
        pl.semaphore_signal(barrier, inc=1, device_id=peer, device_id_type=MESH)

    half = out.shape[2] // 2
    mine = pl.ds(pl.multiple_of(c * half, 128), half)
    theirs = pl.ds(pl.multiple_of(o * half, 128), half)
    kcols = pl.ds(pl.multiple_of(x * 128, 128), 128)
    vcols = pl.ds(pl.multiple_of(p * 128, 128), 128)
    wrows = pl.ds(pl.multiple_of(c * 128, 128), 128)
    loads = [
        (tokens.at[0], tokv),
        (ld, ldv),
        (rd, rdv),
        (qw, qwv),
        (pd, wv.at[:, 0:128]),
        (ku.at[:, kcols], kuv),
        (vu.at[:, vcols], vuv),
        (pw.at[pl.ds(p * 2, 2)], pwv),
        (tab, tabv),
        (ao.at[:, mine], w2.at[0, wrows]),
        (po.at[:, mine], w2.at[1, wrows]),
        (igh, ig),
        (qgh, qg),
        (kgh, kg),
        (psh, ps),
        (agh, ag),
        (pgh, pg),
    ]
    copies = [pltpu.make_async_copy(s, d, dsem.at[i]) for i, (s, d) in enumerate(loads)]
    for i in (0, 11, 1, 2, 5, 6, 12, 13, 3, 4, 8, 7, 9, 10, 14, 15, 16):
        copies[i].start()

    copies[0].wait()
    copies[11].wait()
    source = tokv[...].astype(F32)
    scale = lax.rsqrt(jnp.mean(source * source, axis=1, keepdims=True) + EPS)
    normed = (source * scale * ig[...]).astype(BF)
    nt[p] = normed
    copies[1].wait()
    copies[2].wait()
    latent = dot(normed, ldv[...]).astype(BF).astype(F32)
    rotary = dot(rdv[...], normed, ((1,), (1,))).astype(BF).astype(F32)
    swap = (lax.broadcasted_iota(jnp.int32, (16, ROWS), 0) + c * 16) >= 16
    turned = [jnp.where(swap, rotary[16:32], rotary[:16]), jnp.where(swap, rotary[:16], rotary[16:32])]
    lat = latent * lax.rsqrt(jnp.mean(latent * latent, axis=1, keepdims=True) + EPS)
    swap = (lax.broadcasted_iota(jnp.int32, (ROWS, 128), 0) + c * 2 * ROWS) >= 2 * ROWS
    stacked = jnp.concatenate(
        [jnp.where(swap, lat[:, 128:], lat[:, :128]), jnp.where(swap, lat[:, :128], lat[:, 128:])], axis=0
    )
    xt[z, x, c, 0:128, :] = stacked.T.astype(BF)
    xt[z, x, c, 128:144, :] = jnp.concatenate(turned, axis=1).astype(BF)

    pl.semaphore_wait(barrier, len(peers))

    rows_core, ring_core = c == 0, c == 1
    own = xt.at[z, x]
    piece = xt.at[z, x, c]

    def up(s, k, pair):
        send(pair, pair, usnd.at[lax.rem(s, 2)], urcv.at[s, k], at(zu, x, 1))

    def down(s, k, pair):
        send(pair, pair, dsnd.at[lax.rem(s, 2)], drcv.at[s, k], at(zd, x, 1))

    def other(ssem, sem, j):
        send(xt.at[j], xt.at[j], ssem, orcv.at[sem], at(z, x, 0))

    def goes_up(s):
        return (z - s >= 0) & (z < NS - 1)

    def goes_down(s):
        return (z + s <= 6) | (z + s >= NS)

    @pl.when(rows_core)
    def _():
        send(piece, piece, gsnd.at[0], grcv.at[0, 0], at(z, x, 1))

    send(piece, piece, gsnd.at[0], grcv.at[3, c], at(z, xr, 1))
    send(piece, piece, gsnd.at[0], grcv.at[1, c], at(z, xl, 1))
    send(piece, piece, gsnd.at[0], grcv.at[2, c], at(z, xf, 1))

    def trows(xx, h):
        return nt.at[xx * 2 + h]

    def right(h, i, xx):
        send(trows(xx, h), trows(xx, h), tsnd.at[0], trcv.at[0, i], at(z, xr, 0))

    def left(h, i, xx):
        send(trows(xx, h), trows(xx, h), tsnd.at[0], trcv.at[1, i], at(z, xl, 0))

    send(nt.at[p], nt.at[p], vsnd.at[0], vrcv.at[0], at(z, x, o))

    @pl.when(rows_core)
    def _():
        right(0, 0, x)
        got(trows(x, 1), vsnd.at[0], vrcv.at[0])
        left(1, 1, x)
        right(1, 1, x)
        left(0, 0, x)

    @pl.when(ring_core)
    def _():
        got(piece, gsnd.at[0], grcv.at[0, 0])

        @pl.when(goes_up(0))
        def _():
            up(0, 0, own)

        @pl.when(goes_down(0))
        def _():
            down(0, 0, own)

    for i, w in enumerate((ao, po)):
        send(w.at[:, theirs], w2.at[i, wrows], wsnd.at[0], wrcv.at[0], at(z, x, o))

    copies[5].wait()
    copies[6].wait()
    kut[...] = kuv[...].astype(F32).T.astype(BF)
    vut[...] = vuv[...].astype(F32).T.astype(BF)
    copies[12].wait()
    copies[13].wait()
    qcol[...] = jnp.broadcast_to(qg[...], (128, QK)).T
    kcol[...] = jnp.broadcast_to(kg[...], (128, QK)).T
    acc[...] = jnp.zeros_like(acc)
    copies[3].wait()
    for i in range(qwv.shape[1] // 128):
        cols = slice(i * 128, (i + 1) * 128)
        tile = jnp.concatenate([qwv[:, cols].astype(F32), jnp.zeros((128 - QK, 128), F32)], axis=0)
        wv[cols, 128:256] = tile.T.astype(BF)

    def gathered(rel):
        pair = xt.at[z, xmod(x + rel)]
        for i in (0, 1):
            got(piece, gsnd.at[0], grcv.at[rel, i])
        if rel != 1:

            @pl.when(goes_up(0))
            def _():
                up(0, 4 - rel, pair)

        if rel != 3:

            @pl.when(goes_down(0))
            def _():
                down(0, rel, pair)

    @pl.when(ring_core)
    def _():
        gathered(1)
        gathered(3)

    copies[8].wait()

    def rotate(a, b, first):
        cosine = tabv[0:16, pl.ds(first, a.shape[1])]
        sine = tabv[16:32, pl.ds(first, a.shape[1])]
        return a * cosine - b * sine, b * cosine + a * sine

    def expand(j):
        lane = lax.broadcasted_iota(jnp.int32, (144, 128), 1)
        low, high = [], []
        for xx in range(NX):
            p0 = xt[j, xx, 0].astype(F32)
            p1 = xt[j, xx, 1].astype(F32)
            low.append(jnp.where(lane < 64, p0, p1))
            high.append(pltpu.roll(jnp.where(lane < 64, p1, p0), 64, 1))
        low = jnp.concatenate(low, axis=1)
        high = jnp.concatenate(high, axis=1)
        lat2 = jnp.concatenate([low[:128].astype(BF), high[:128].astype(BF)], axis=0)
        plain = dot(kut[pl.ds(pl.multiple_of(c * 64, 64), 64), :], lat2)
        vtv[j] = dot(vut[...], lat2).astype(BF)
        a, b = low[128:144], high[128:144]
        total = jnp.sum(plain * plain, axis=0, keepdims=True)
        total = total + jnp.sum(a * a + b * b, axis=0, keepdims=True)
        factor = lax.rsqrt(total * (1.0 / QK) + EPS)
        gain = kcol[:, 0:1]
        first = pl.multiple_of(j * BLOCK, 128)
        a, b = rotate(a * factor * gain[64:80], b * factor * gain[80:96], first)
        ktv[j, 0:64, :] = (plain * factor * gain[0:64]).astype(BF)
        ktv[j, 64:80, :] = a.astype(BF)
        ktv[j, 80:96, :] = b.astype(BF)
        ktv[j, QK:128, :] = jnp.zeros((128 - QK, BLOCK), BF)

    def attend(j, masked):
        both = jnp.concatenate([vtv[j], jnp.ones((128, BLOCK), BF)], axis=0)
        weight = jnp.exp2(dot(qv[...], ktv[j]))
        if masked:
            qpos = lax.broadcasted_iota(jnp.int32, weight.shape, 0)
            kpos = lax.broadcasted_iota(jnp.int32, weight.shape, 1)
            weight = jnp.where(kpos <= qpos, weight, 0.0)
        acc[...] += dot(weight.astype(BF), both, ((1,), (1,)))

    def block_of(u):
        return jnp.where(lax.rem(u, 2) == 1, z - (u + 1) // 2, z + u // 2 - NS)

    def project(chips):
        rows = [nt[2 * t + i] for t in chips for i in (0, 1)]
        both = dot(jnp.concatenate(rows, axis=0), wv[...])
        raws = both[:, 128:].T[:QK]
        for i, t in enumerate(chips):
            spot = pl.ds(pl.multiple_of(t * 128, 128), 128)
            poolin[pl.ds(pl.multiple_of(t * 128 + RIM, 8), 128), :] = (
                both[i * 128 : (i + 1) * 128, :128].astype(BF).astype(F32)
            )
            raw = raws[:, i * 128 : (i + 1) * 128]
            total = jnp.sum(raw * raw, axis=0, keepdims=True)
            normal = raw * lax.rsqrt(total * (1.0 / QK) + EPS) * qcol[:, 0:1] * SCALE
            first = pl.multiple_of(z * BLOCK + t * 128, 128)
            a, b = rotate(normal[64:80], normal[80:96], first)
            full = jnp.concatenate([normal[:64], a, b, jnp.zeros((32, 128), F32)], axis=0)
            qv[spot, :] = full.T.astype(BF)

    def sumsq(values):
        return dot(jnp.ones((8, 128), F32), values * values, ((1,), (1,)), lax.Precision.HIGHEST)

    def spread(totals, start):
        sub = lax.broadcasted_iota(jnp.int32, (8, 128), 0)
        packed = jnp.zeros((8, 128), F32)
        for t in range(NX):
            packed = jnp.where(sub == start + t, totals[:, t * 128 : (t + 1) * 128], packed)
        return packed

    def pool():
        @pl.when(z > 0)
        def _():
            got(halo, hsnd.at[0], hrcv.at[0])

        poolin[0:RIM, :] = jnp.where(z > 0, halo[...].astype(F32), 0.0)
        values = poolin[...]
        two = values + pltpu.roll(values, 1, 0)
        four = two + pltpu.roll(two, 2, 0)
        eight = four + pltpu.roll(four, 4, 0)
        sixteen = eight + pltpu.roll(eight, 8, 0)
        lane = lax.broadcasted_iota(jnp.int32, (BLOCK, 128), 1)
        wide = c == 1
        left = jnp.where(wide ^ (x < 0), eight, two)[RIM:]
        right = jnp.where(wide ^ (x < 0), sixteen, four)[RIM:]
        total = jnp.where(lane < 64, left, right)
        base = jnp.where(wide, 8.0, 2.0)
        window = jnp.where(lane < 64, base, base * 2.0)
        count = (lax.broadcasted_iota(jnp.int32, (BLOCK, 128), 0) + (z * BLOCK + 1)).astype(F32)
        mean = (total / jnp.minimum(count, window) - values[RIM:]).astype(BF)
        zero = jnp.zeros((64, 64), F32)
        w0 = jnp.concatenate([pwv[0].astype(F32), zero], axis=1)
        w1 = jnp.concatenate([zero, pwv[1].astype(F32)], axis=1)
        copies[14].wait()
        copies[16].wait()
        pooled = dot(mean, jnp.concatenate([w0, w1], axis=0).astype(BF)) * ps[...]
        ssq[p] = spread(sumsq(pooled), 4)
        px[c] = (pooled * pg[...]).astype(BF)
        send(px.at[c], px.at[c], psnd.at[0], prcv.at[0], at(z, x, o))

    def pool_rows(t, h):
        rows = pl.ds(pl.multiple_of(t * 128, 128), 128)
        both = jnp.concatenate([px[0, rows], px[1, rows]], axis=1)
        return dot(both, w2[1, :, h * 512 : (h + 1) * 512])

    def far_pool():
        got(px.at[o], psnd.at[0], prcv.at[0])
        for i in (0, 1):
            copies[9 + i].wait()
        got(w2.at[:, pl.ds(pl.multiple_of(o * 128, 128), 128)], wsnd.at[0], wrcv.at[0])
        for h in (0, 1):
            fpool[h] = pool_rows(xf, h).astype(BF)

    def send_far_pool(i):
        rows = pl.ds(pl.multiple_of(i * 32, 32), 32)
        for h, xx in ((0, xr), (1, xl)):
            send(fpool.at[h, rows], fgot.at[h, rows], fsnd.at[0], frcv.at[h], at(z, xx, c))

    own_block = xt.at[z]

    def piece_up(s, k):
        return xt.at[zmod(z - s), xmod(x - k)]

    def piece_down(s, k):
        return xt.at[zmod(z + s), xmod(x + k)]

    def from_below(s):
        return z - s >= 0

    def from_above(s):
        return z + s >= NS

    def side_left(s):
        pair = piece_up(s, 0)

        @pl.when(s >= 3)
        def _():
            sent(own, ysnd.at[0, lax.rem(s, 2)], yrcv.at[0, 0])

        send(pair, pair, ysnd.at[0, lax.rem(s, 2)], yrcv.at[0, s - 1], at(z, xl, 1))

    def side_right(s):
        pair = piece_down(s, 0)

        @pl.when((s >= 3) & from_above(s - 2))
        def _():
            sent(own, ysnd.at[1, lax.rem(s, 2)], yrcv.at[1, 0])

        send(pair, pair, ysnd.at[1, lax.rem(s, 2)], yrcv.at[1, s - 1], at(z, xr, 1))

    def slot(s, k):
        n = 3 * s - 3 + k

        def slots(*numbers):
            def run(work):
                here = [s == v // 3 + 1 for v in numbers if v % 3 == k]
                if here:
                    pl.when(functools.reduce(jnp.logical_or, here))(work)

            return run


        @pl.when(ring_core & from_below(s) & (s < 9))
        def _():
            pair = piece_up(s, k)
            got(pair, usnd.at[0], urcv.at[s - 1, k])

            if k == 0:

                @pl.when((s >= 2) & goes_up(s - 2) & (s < 8))
                def _():
                    sent(xt.at[z, 0:3], usnd.at[lax.rem(s, 2)], urcv.at[0, 0])

            @pl.when((s < 8) & (z < NS - 1))
            def _():
                up(s, k, pair)

            if k == 0:

                @pl.when(s >= 3)
                def _():
                    side_left(s)

        @pl.when(ring_core & goes_down(s) & (s < 8))
        def _():
            pair = piece_down(s, k)
            got(pair, dsnd.at[0], drcv.at[s - 1, k])

            @pl.when(s < 7)
            def _():
                if k == 0:

                    @pl.when((s >= 2) & goes_down(s - 2))
                    def _():
                        sent(xt.at[z, 0:3], dsnd.at[lax.rem(s, 2)], drcv.at[0, 0])

                down(s, k, pair)

            if k == 0:

                @pl.when((s >= 3) & from_above(s))
                def _():
                    side_right(s)

        @slots(0)
        def _():
            @pl.when(ring_core)
            def _():
                gathered(2)
                send(piece, piece, nsnd.at[0], orcv.at[15], at(z, x, 0))
                for i, xx in enumerate((xr, xl, xf)):
                    pair = xt.at[z, xx]
                    send(pair, pair, nsnd.at[0], orcv.at[16 + i], at(z, x, 0))

        @slots(4, 5)
        def _():
            @pl.when(ring_core)
            def _():
                @pl.when(from_below(n - 3))
                def _():
                    side_left(n - 3)

                @pl.when(from_above(n - 3))
                def _():
                    side_right(n - 3)

        @slots(8)
        def _():
            @pl.when(ring_core)
            def _():
                sides(1)
                sides(2)

        if k == 0:

            @pl.when(ring_core & (s >= 4))
            def _():
                sides(s - 1)

        @slots(0)
        def _():
            @pl.when(rows_core)
            def _():
                got(trows(xl, 0), tsnd.at[0], trcv.at[0, 0])
                right(0, 2, xl)
                got(trows(xr, 1), tsnd.at[0], trcv.at[1, 1])
                left(1, 2, xr)

        @slots(3)
        def _():
            @pl.when(rows_core)
            def _():
                got(xt.at[z, x, 1], nsnd.at[0], orcv.at[15])
                for i, xx in enumerate((xr, xl, xf)):
                    got(xt.at[z, xx], nsnd.at[0], orcv.at[16 + i])

            expand(z)

        def pass_on(i, xx):
            block = nt.at[pl.ds(xx * 2, 2)]
            send(block, block, vsnd.at[0], vrcv.at[i], at(z, x, 1))

        def passed(i, xx):
            got(nt.at[pl.ds(xx * 2, 2)], vsnd.at[0], vrcv.at[i])

        @slots(4)
        def _():
            @pl.when(rows_core)
            def _():
                got(trows(xl, 1), tsnd.at[0], trcv.at[0, 1])
                pass_on(1, xl)
                got(trows(xr, 0), tsnd.at[0], trcv.at[1, 0])
                pass_on(2, xr)

        @slots(6)
        def _():
            copies[4].wait()

            @pl.when(ring_core)
            def _():
                got(trows(x, 0), vsnd.at[0], vrcv.at[0])
                passed(1, xl)
                passed(2, xr)

            project((x, xl, xr))

        @slots(7)
        def _():
            @pl.when(rows_core)
            def _():
                got(trows(xf, 0), tsnd.at[0], trcv.at[0, 2])
                got(trows(xf, 1), tsnd.at[0], trcv.at[1, 2])
                pass_on(3, xf)

        @slots(9)
        def _():
            @pl.when(ring_core)
            def _():
                passed(3, xf)

            project((xf,))
            rim[...] = poolin[BLOCK:, :].astype(BF)

            @pl.when(z < NS - 1)
            def _():
                send(rim, halo, hsnd.at[0], hrcv.at[0], at(zu, x, c))

        @slots(START)
        def _():
            attend(z, True)

        @slots(START + 2)
        def _():
            copies[7].wait()
            pool()

        @slots(START + 6)
        def _():
            far_pool()

        @slots(START + 6, START + 7, START + 9, START + 10)
        def _():
            send_far_pool(jnp.where(n < START + 8, n - (START + 6), n - (START + 7)))

        e = jnp.where(n <= 21, n - 9, jnp.where(n < 26, n - 10, 15))
        je = block_of(e)
        due = (n >= 10) & (n != 22) & (n != 25) & (je >= 0)
        ja = block_of(jnp.where(n <= 22, n - 10, n - 11))
        ripe = (n >= 11) & (n != 23) & (n != 26) & (ja >= 0)

        @pl.when(due & rows_core)
        def _():
            got(xt.at[je], nsnd.at[0], orcv.at[e - 1])

        @pl.when(due & ripe)
        def _():
            attend(ja, False)
            expand(je)

        @pl.when(due != ripe)
        def _():
            @pl.when(due)
            def _():
                expand(je)

            @pl.when(ripe)
            def _():
                attend(ja, False)

    def step(s, carry):
        for k in range(3):
            slot(s, k)
        return carry

    def sides(s):
        @pl.when(from_below(s))
        def _():
            pair = xt.at[zmod(z - s), xr]
            got(pair, ysnd.at[0, 0], yrcv.at[0, s - 1])
            ssem = osnd.at[0, lax.rem(s, 2)]

            @pl.when(s >= 3)
            def _():
                sent(own_block, ssem, orcv.at[15])

            other(ssem, 2 * s - 2, zmod(z - s))

        @pl.when(from_above(s) & (s < 8))
        def _():
            pair = xt.at[zmod(z + s), xl]
            got(pair, ysnd.at[1, 0], yrcv.at[1, s - 1])
            ssem = osnd.at[1, lax.rem(s, 2)]

            @pl.when((s >= 3) & from_above(s - 2))
            def _():
                sent(own_block, ssem, orcv.at[15])

            other(ssem, 2 * s - 1, zmod(z + s))

    lax.fori_loop(1, 10, step, 0)

    @pl.when(z >= 8)
    def _():
        attend(z - 8, False)

    copies[15].wait()
    attended = acc[:, :128] / acc[:, 128:]
    ssq[p] = ssq[p] + spread(sumsq(attended), 0)
    ax[c] = (attended * ag[...]).astype(BF)
    send(ax.at[c], ax.at[c], psnd.at[1], prcv.at[1], at(z, x, o))
    for xx, cc in [(xf, c), (xf, o), (xr, c), (xl, c), (xr, o), (xl, o), (x, o)]:
        send(ssq.at[p], ssq.at[p], ssnd.at[0], srcv.at[0], at(z, xx, cc))
    for t in (xr, xl, x):
        for h in (0, 1):
            bpart[t, h] = pool_rows(t, h)

    def mixed_rows(t, h):
        rows = pl.ds(pl.multiple_of(t * 128, 128), 128)
        both = jnp.concatenate([ax[0, rows], ax[1, rows]], axis=1)
        return dot(both, w2[0, :, h * 512 : (h + 1) * 512])

    got(ax.at[o], psnd.at[1], prcv.at[1])
    for h in (0, 1):
        part[xf, h] = mixed_rows(xf, h).astype(BF)
    send(part.at[xf, 0], far.at[0], rsnd.at[0], rrcv.at[0], at(z, xr, c))
    send(part.at[xf, 1], far.at[1], rsnd.at[0], rrcv.at[1], at(z, xl, c))
    got(ssq.at[0:7], ssnd.at[0], srcv.at[0])
    total = ssq[0]
    for i in range(1, 8):
        total = total + ssq[i]
    factor = lax.rsqrt(total * (1.0 / 1024.0) + EPS)
    fcol[...] = jnp.concatenate([factor, jnp.zeros((120, 128), F32)], axis=0).T

    lane = lax.broadcasted_iota(jnp.int32, (128, 128), 1)

    def pick(k):
        return jnp.sum(jnp.where(lane == k, fcol[...], 0.0), axis=1, keepdims=True)

    def partial(t, hs):
        fa, fp = pick(t), pick(t + 4)
        for h in hs:
            part[t, h] = (mixed_rows(t, h) * fa + bpart[t, h] * fp).astype(BF)

    def combined(t, h):
        term = mixed_rows(t, h) + far[h].astype(F32)
        base = bpart[t, h] + fgot[h].astype(F32)
        part[t, h] = (term * pick(t) + base * pick(t + 4)).astype(BF)

    def rrows(cc):
        return pl.ds(pl.multiple_of(cc * ROWS, ROWS), ROWS)

    def to_right(h, i):
        for cc in (0, 1):
            send(part.at[xr, h, rrows(cc)], fin.at[c, i], esnd.at[0], ercv.at[0], at(z, xr, cc))

    def to_left(h, i):
        for cc in (0, 1):
            send(part.at[xl, h, rrows(cc)], fin.at[c, i], esnd.at[0], ercv.at[0], at(z, xl, cc))

    partial(xr, (1,))
    to_right(1, 2)
    partial(xl, (0,))
    to_left(0, 0)
    partial(x, (0, 1))
    send(part.at[x, :, rrows(o)], ownp, rsnd.at[1], rrcv.at[2], at(z, x, o))
    for i in (0, 1):
        got(fgot.at[i], fsnd.at[0], frcv.at[i])
    got(far.at[0], rsnd.at[0], rrcv.at[0])
    combined(xr, 0)
    to_right(0, 1)
    got(far.at[1], rsnd.at[0], rrcv.at[1])
    combined(xl, 1)
    to_left(1, 3)

    got(ownp, rsnd.at[1], rrcv.at[2])
    got(fin, esnd.at[0], ercv.at[0])
    for h in (0, 1):
        for sub in (0, 1):
            mixed = fin[h, 2 * sub].astype(F32) + fin[h, 2 * sub + 1].astype(F32)
            here = jnp.where(c == h, part[x, sub, rrows(c)].astype(F32), ownp[sub].astype(F32))
            lo = h * 1024 + sub * 512
            out[0, :, lo : lo + 512] = (mixed + here).astype(BF)

    @pl.when(rows_core)
    def _():
        sent(xt.at[z, 0:2], gsnd.at[0], grcv.at[0, 0])
        sent(nt.at[0:6], tsnd.at[0], trcv.at[0, 0])
        sent(nt.at[0:7], vsnd.at[0], vrcv.at[0])

    @pl.when(ring_core)
    def _():
        sent(xt.at[z, 0:3, 0], gsnd.at[0], grcv.at[0, 0])
        sent(nt.at[p], vsnd.at[0], vrcv.at[0])
        sent(xt.at[0:7, 0, 0], nsnd.at[0], orcv.at[15])

    sent(w2.at[:, wrows], wsnd.at[0], wrcv.at[0])
    for i in (0, 1):
        sent(px.at[c], psnd.at[i], prcv.at[i])
    sent(far, rsnd.at[0], rrcv.at[0])
    sent(ownp, rsnd.at[1], rrcv.at[2])
    sent(fpool, fsnd.at[0], frcv.at[0])
    sent(ssq.at[0:7], ssnd.at[0], srcv.at[0])
    sent(fin, esnd.at[0], ercv.at[0])

    @pl.when(z < NS - 1)
    def _():
        sent(rim, hsnd.at[0], hrcv.at[0])

    def drain(s, carry):
        odd = lax.rem(s, 2)
        other_odd = 1 - odd

        @pl.when(goes_up(s) & jnp.logical_not(goes_up(s + 2) & (s < 6)))
        def _():
            sent(xt.at[z, 0:3], usnd.at[odd], urcv.at[0, 0])

        @pl.when(goes_down(s) & (s < 7) & jnp.logical_not(goes_down(s + 2) & (s < 5)))
        def _():
            sent(xt.at[z, 0:3], dsnd.at[odd], drcv.at[0, 0])

        @pl.when(from_below(s + 1) & jnp.logical_not(from_below(s + 3) & (s < 6)))
        def _():
            sent(own, ysnd.at[0, other_odd], yrcv.at[0, 0])
            sent(own_block, osnd.at[0, other_odd], orcv.at[15])

        @pl.when(from_above(s + 1) & (s < 7) & jnp.logical_not(from_above(s + 3) & (s < 5)))
        def _():
            sent(own, ysnd.at[1, other_odd], yrcv.at[1, 0])
            sent(own_block, osnd.at[1, other_odd], orcv.at[15])

        return carry

    @pl.when(ring_core)
    def _():
        lax.fori_loop(0, 8, drain, 0)


def rope_table(length):
    halfway = 16
    inv = (1.0 / np.float32(THETA) ** (np.arange(halfway, dtype=np.float32) / np.float32(halfway))).astype(np.float32)
    angle = (np.arange(length, dtype=np.float32)[None, :] * inv[:, None]).astype(np.float32).astype(np.float64)
    return np.concatenate([np.cos(angle), np.sin(angle)], axis=0).astype(np.float32)


def local(
    tokens, input_gain, query_weight, latent_down, rotary_down, pool_down, key_up, value_up,
    query_gain, key_gain, pool_weight, pool_scale, attention_gain, pool_gain, attention_out, pool_out,
):
    width = tokens.shape[2]
    table = jnp.asarray(rope_table(NS * BLOCK))
    hbm = pl.BlockSpec(memory_space=pl.ANY)
    vmem = pl.BlockSpec(memory_space=pltpu.VMEM)
    V = pltpu.VMEM
    D = pltpu.SemaphoreType.DMA
    half = width // 2
    scratch = [
        V((ROWS, width), BF), V((1, width), F32), V((8, ROWS, width), BF), V((QK, width), BF),
        V((width, 256), BF), V((32, width), BF), V((width, 256), BF), V((256, 128), BF), V((256, 128), BF),
        V((1, QK), F32), V((1, QK), F32), V((2, 64, 64), BF), V((1, 128), F32), V((1, 128), F32),
        V((1, 128), F32), V((2, 256, half), BF), V((32, NS * BLOCK), F32),
        V((NS, NX, 2, 144, 128), BF), V((128, 256), BF), V((128, 256), BF), V((BLOCK, 128), BF),
        V((NS, 128, BLOCK), BF), V((NS, 128, BLOCK), BF), V((BLOCK, 256), F32),
        V((QK, 128), F32), V((QK, 128), F32),
        V((RIM, 128), BF), V((RIM, 128), BF), V((BLOCK + RIM, 128), F32), V((2, BLOCK, 128), BF),
        V((2, BLOCK, 128), BF), V((NX, 2, 128, half // 2), F32),
        V((8, 8, 128), F32), V((NX, 2, 128, half // 2), BF), V((2, 128, half // 2), BF),
        V((2, 4, ROWS, half // 2), BF), V((2, ROWS, half // 2), BF), V((128, 128), F32), V((2, 128, half // 2), BF), V((2, 128, half // 2), BF),
        D((17,)),
        D((2,)), D((8, 3)), D((2,)), D((7, 3)), D((2, 2)), D((2, 8)), D((1,)), D((4, 2)),
        D((2, 2)), D((19,)), D((1,)), D((2,)), D((2,)),
        D((1,)), D((2, 3)), D((1,)), D((4,)), D((1,)), D((1,)), D((1,)), D((1,)),
        D((1,)), D((1,)), D((1,)), D((1,)), D((2,)), D((3,)), D((1,)), D((2,)),
    ]
    args = (
        tokens, input_gain.reshape(1, -1), query_weight.T, latent_down, rotary_down.T, pool_down, key_up, value_up,
        query_gain.reshape(1, -1), key_gain.reshape(1, -1), pool_weight, pool_scale.reshape(1, -1),
        attention_gain.reshape(1, -1), pool_gain.reshape(1, -1), attention_out, pool_out, table,
    )
    specs = [hbm] * 17
    return pl.pallas_call(
        kernel,
        out_shape=pltpu.VMEM(tokens.shape, BF),
        in_specs=specs,
        out_specs=vmem,
        scratch_shapes=scratch,
        compiler_params=pltpu.CompilerParams(
            collective_id=0, has_side_effects=True, vmem_limit_bytes=60 * 1024 * 1024
        ),
    )(*args)


def solution(mesh):
    placed = (
        P("fs", ("sp", "tp"), None), P(), P(None, "tp"), P(), P(), P(None, "tp"), P(), P(),
        P(), P(), P(), P("tp"), P("tp"), P("tp"), P("tp", None), P("tp", None),
    )
    return jax.shard_map(
        local, mesh=mesh, in_specs=placed, out_specs=P("fs", ("sp", "tp"), None), check_vma=False
    )
```

```python
import functools
import math

import jax
import jax.numpy as jnp
import numpy as np
from jax import lax
from jax.experimental import pallas as pl
from jax.experimental.pallas import tpu as pltpu
from jax.sharding import PartitionSpec as P

MESH = pl.DeviceIdType.MESH
BF = jnp.bfloat16
F32 = jnp.float32

EPS = 1e-06
THETA = 10000.0
QK = 96
SCALE = math.log2(math.e) / math.sqrt(QK)
NX = 4
NS = 16
BLOCK = 512
ROWS = 64
RIM = 16
START = 11


def dot(a, b, dims=((1,), (0,)), precision=None):
    return lax.dot_general(a, b, (dims, ((), ())), preferred_element_type=F32, precision=precision)


def kernel(
    tokens, igh, qw, ld, rd, pd, ku, vu, qgh, kgh, pw, psh, agh, pgh, ao, po, tab,
    out,
    tokv, ig, nt, qwv, ldv, rdv, wv, kuv, vuv, qg, kg, pwv, ps, ag, pg, w2, tabv,
    xt, kut, vut, qv, ktv, vtv, acc, qcol, kcol, rim, halo, poolin, px, ax, bpart,
    ssq, part, far, fin, ownp, fcol, fpool, fgot,
    dsem, usnd, urcv, dsnd, drcv, ysnd, yrcv, gsnd, grcv, osnd, orcv, nsnd, psnd, prcv,
    tsnd, trcv, vsnd, vrcv, wsnd, wrcv, hsnd, hrcv, esnd, ercv, ssnd, srcv, rsnd, rrcv, fsnd, frcv,
):
    z = lax.axis_index("sp")
    fs = lax.axis_index("fs")
    p = lax.axis_index("tp")
    c = lax.rem(p, 2)
    x = p // 2
    o = 1 - c

    def zmod(v):
        return lax.rem(v + 2 * NS, NS)

    def xmod(v):
        return lax.rem(v + 2 * NX, NX)

    def at(zz, xx, cc):
        return (zz, fs, xx * 2 + cc)

    xr, xl, xf = xmod(x + 1), xmod(x - 1), xmod(x + 2)
    zu, zd = zmod(z + 1), zmod(z - 1)

    def send(src, dst, ssem, rsem, dev):
        copy = pltpu.make_async_remote_copy(
            src_ref=src, dst_ref=dst, send_sem=ssem, recv_sem=rsem, device_id=dev, device_id_type=MESH
        )
        copy.start()

    def got(dst, ssem, rsem):
        pltpu.make_async_remote_copy(
            src_ref=dst, dst_ref=dst, send_sem=ssem, recv_sem=rsem,
            device_id=at(z, x, o), device_id_type=MESH,
        ).wait_recv()

    def sent(src, ssem, rsem):
        pltpu.make_async_remote_copy(
            src_ref=src, dst_ref=src, send_sem=ssem, recv_sem=rsem,
            device_id=at(z, x, o), device_id_type=MESH,
        ).wait_send()

    barrier = pltpu.get_barrier_semaphore()
    peers = [at(z, x, o), at(zu, x, c), at(zd, x, c)]
    peers += [at(z, xx, cc) for xx in (xr, xl, xf) for cc in (c, o)]
    for peer in peers:
        pl.semaphore_signal(barrier, inc=1, device_id=peer, device_id_type=MESH)

    half = out.shape[2] // 2
    mine = pl.ds(pl.multiple_of(c * half, 128), half)
    theirs = pl.ds(pl.multiple_of(o * half, 128), half)
    kcols = pl.ds(pl.multiple_of(x * 128, 128), 128)
    vcols = pl.ds(pl.multiple_of(p * 128, 128), 128)
    wrows = pl.ds(pl.multiple_of(c * 128, 128), 128)
    loads = [
        (tokens.at[0], tokv),
        (ld, ldv),
        (rd, rdv),
        (qw, qwv),
        (pd, wv.at[:, 0:128]),
        (ku.at[:, kcols], kuv),
        (vu.at[:, vcols], vuv),
        (pw.at[pl.ds(p * 2, 2)], pwv),
        (tab, tabv),
        (ao.at[:, mine], w2.at[0, wrows]),
        (po.at[:, mine], w2.at[1, wrows]),
        (igh, ig),
        (qgh, qg),
        (kgh, kg),
        (psh, ps),
        (agh, ag),
        (pgh, pg),
    ]
    copies = [pltpu.make_async_copy(s, d, dsem.at[i]) for i, (s, d) in enumerate(loads)]
    for i in (0, 11, 1, 2, 5, 6, 12, 13, 3, 4, 8, 7, 9, 10, 14, 15, 16):
        copies[i].start()

    copies[0].wait()
    copies[11].wait()
    source = tokv[...].astype(F32)
    scale = lax.rsqrt(jnp.mean(source * source, axis=1, keepdims=True) + EPS)
    normed = (source * scale * ig[...]).astype(BF)
    nt[p] = normed
    copies[1].wait()
    copies[2].wait()
    latent = dot(normed, ldv[...]).astype(BF).astype(F32)
    rotary = dot(rdv[...], normed, ((1,), (1,))).astype(BF).astype(F32)
    swap = (lax.broadcasted_iota(jnp.int32, (16, ROWS), 0) + c * 16) >= 16
    turned = [jnp.where(swap, rotary[16:32], rotary[:16]), jnp.where(swap, rotary[:16], rotary[16:32])]
    lat = latent * lax.rsqrt(jnp.mean(latent * latent, axis=1, keepdims=True) + EPS)
    swap = (lax.broadcasted_iota(jnp.int32, (ROWS, 128), 0) + c * 2 * ROWS) >= 2 * ROWS
    stacked = jnp.concatenate(
        [jnp.where(swap, lat[:, 128:], lat[:, :128]), jnp.where(swap, lat[:, :128], lat[:, 128:])], axis=0
    )
    xt[z, x, c, 0:128, :] = stacked.T.astype(BF)
    xt[z, x, c, 128:144, :] = jnp.concatenate(turned, axis=1).astype(BF)

    pl.semaphore_wait(barrier, len(peers))

    rows_core, ring_core = c == 0, c == 1
    own = xt.at[z, x]
    piece = xt.at[z, x, c]

    def up(s, k, pair):
        send(pair, pair, usnd.at[lax.rem(s, 2)], urcv.at[s, k], at(zu, x, 1))

    def down(s, k, pair):
        send(pair, pair, dsnd.at[lax.rem(s, 2)], drcv.at[s, k], at(zd, x, 1))

    def other(ssem, sem, j):
        send(xt.at[j], xt.at[j], ssem, orcv.at[sem], at(z, x, 0))

    def goes_up(s):
        return (z - s >= 0) & (z < NS - 1)

    def goes_down(s):
        return (z + s <= 6) | (z + s >= NS)

    @pl.when(rows_core)
    def _():
        send(piece, piece, gsnd.at[0], grcv.at[0, 0], at(z, x, 1))

    send(piece, piece, gsnd.at[0], grcv.at[3, c], at(z, xr, 1))
    send(piece, piece, gsnd.at[0], grcv.at[1, c], at(z, xl, 1))
    send(piece, piece, gsnd.at[0], grcv.at[2, c], at(z, xf, 1))

    def trows(xx, h):
        return nt.at[xx * 2 + h]

    def right(h, i, xx):
        send(trows(xx, h), trows(xx, h), tsnd.at[0], trcv.at[0, i], at(z, xr, 0))

    def left(h, i, xx):
        send(trows(xx, h), trows(xx, h), tsnd.at[0], trcv.at[1, i], at(z, xl, 0))

    send(nt.at[p], nt.at[p], vsnd.at[0], vrcv.at[0], at(z, x, o))

    @pl.when(rows_core)
    def _():
        right(0, 0, x)
        got(trows(x, 1), vsnd.at[0], vrcv.at[0])
        left(1, 1, x)
        right(1, 1, x)
        left(0, 0, x)

    @pl.when(ring_core)
    def _():
        got(piece, gsnd.at[0], grcv.at[0, 0])

        @pl.when(goes_up(0))
        def _():
            up(0, 0, own)

        @pl.when(goes_down(0))
        def _():
            down(0, 0, own)

    for i, w in enumerate((ao, po)):
        send(w.at[:, theirs], w2.at[i, wrows], wsnd.at[0], wrcv.at[0], at(z, x, o))

    copies[5].wait()
    copies[6].wait()
    kut[...] = kuv[...].astype(F32).T.astype(BF)
    vut[...] = vuv[...].astype(F32).T.astype(BF)
    copies[12].wait()
    copies[13].wait()
    qcol[...] = jnp.broadcast_to(qg[...], (128, QK)).T
    kcol[...] = jnp.broadcast_to(kg[...], (128, QK)).T
    acc[...] = jnp.zeros_like(acc)
    copies[3].wait()
    for i in range(qwv.shape[1] // 128):
        cols = slice(i * 128, (i + 1) * 128)
        tile = jnp.concatenate([qwv[:, cols].astype(F32), jnp.zeros((128 - QK, 128), F32)], axis=0)
        wv[cols, 128:256] = tile.T.astype(BF)

    def gathered(rel):
        pair = xt.at[z, xmod(x + rel)]
        for i in (0, 1):
            got(piece, gsnd.at[0], grcv.at[rel, i])
        if rel != 1:

            @pl.when(goes_up(0))
            def _():
                up(0, 4 - rel, pair)

        if rel != 3:

            @pl.when(goes_down(0))
            def _():
                down(0, rel, pair)

    @pl.when(ring_core)
    def _():
        gathered(1)
        gathered(3)
        gathered(2)

    copies[8].wait()

    def rotate(a, b, first):
        cosine = tabv[0:16, pl.ds(first, a.shape[1])]
        sine = tabv[16:32, pl.ds(first, a.shape[1])]
        return a * cosine - b * sine, b * cosine + a * sine

    def expand(j):
        lane = lax.broadcasted_iota(jnp.int32, (144, 128), 1)
        low, high = [], []
        for xx in range(NX):
            p0 = xt[j, xx, 0].astype(F32)
            p1 = xt[j, xx, 1].astype(F32)
            low.append(jnp.where(lane < 64, p0, p1))
            high.append(pltpu.roll(jnp.where(lane < 64, p1, p0), 64, 1))
        low = jnp.concatenate(low, axis=1)
        high = jnp.concatenate(high, axis=1)
        lat2 = jnp.concatenate([low[:128].astype(BF), high[:128].astype(BF)], axis=0)
        plain = dot(kut[pl.ds(pl.multiple_of(c * 64, 64), 64), :], lat2)
        vtv[j] = dot(vut[...], lat2).astype(BF)
        a, b = low[128:144], high[128:144]
        total = jnp.sum(plain * plain, axis=0, keepdims=True)
        total = total + jnp.sum(a * a + b * b, axis=0, keepdims=True)
        factor = lax.rsqrt(total * (1.0 / QK) + EPS)
        gain = kcol[:, 0:1]
        first = pl.multiple_of(j * BLOCK, 128)
        a, b = rotate(a * factor * gain[64:80], b * factor * gain[80:96], first)
        ktv[j, 0:64, :] = (plain * factor * gain[0:64]).astype(BF)
        ktv[j, 64:80, :] = a.astype(BF)
        ktv[j, 80:96, :] = b.astype(BF)
        ktv[j, QK:128, :] = jnp.zeros((128 - QK, BLOCK), BF)

    def attend(j, masked):
        both = jnp.concatenate([vtv[j], jnp.ones((128, BLOCK), BF)], axis=0)
        weight = jnp.exp2(dot(qv[...], ktv[j]))
        if masked:
            qpos = lax.broadcasted_iota(jnp.int32, weight.shape, 0)
            kpos = lax.broadcasted_iota(jnp.int32, weight.shape, 1)
            weight = jnp.where(kpos <= qpos, weight, 0.0)
        acc[...] += dot(weight.astype(BF), both, ((1,), (1,)))

    def block_of(u):
        return jnp.where(lax.rem(u, 2) == 1, z - (u + 1) // 2, z + u // 2 - NS)

    def project(chips):
        rows = [nt[2 * t + i] for t in chips for i in (0, 1)]
        both = dot(jnp.concatenate(rows, axis=0), wv[...])
        raws = both[:, 128:].T[:QK]
        for i, t in enumerate(chips):
            spot = pl.ds(pl.multiple_of(t * 128, 128), 128)
            poolin[pl.ds(pl.multiple_of(t * 128 + RIM, 8), 128), :] = (
                both[i * 128 : (i + 1) * 128, :128].astype(BF).astype(F32)
            )
            raw = raws[:, i * 128 : (i + 1) * 128]
            total = jnp.sum(raw * raw, axis=0, keepdims=True)
            normal = raw * lax.rsqrt(total * (1.0 / QK) + EPS) * qcol[:, 0:1] * SCALE
            first = pl.multiple_of(z * BLOCK + t * 128, 128)
            a, b = rotate(normal[64:80], normal[80:96], first)
            full = jnp.concatenate([normal[:64], a, b, jnp.zeros((32, 128), F32)], axis=0)
            qv[spot, :] = full.T.astype(BF)

    def sumsq(values):
        return dot(jnp.ones((8, 128), F32), values * values, ((1,), (1,)), lax.Precision.HIGHEST)

    def spread(totals, start):
        sub = lax.broadcasted_iota(jnp.int32, (8, 128), 0)
        packed = jnp.zeros((8, 128), F32)
        for t in range(NX):
            packed = jnp.where(sub == start + t, totals[:, t * 128 : (t + 1) * 128], packed)
        return packed

    def pool():
        @pl.when(z > 0)
        def _():
            got(halo, hsnd.at[0], hrcv.at[0])

        poolin[0:RIM, :] = jnp.where(z > 0, halo[...].astype(F32), 0.0)
        values = poolin[...]
        two = values + pltpu.roll(values, 1, 0)
        four = two + pltpu.roll(two, 2, 0)
        eight = four + pltpu.roll(four, 4, 0)
        sixteen = eight + pltpu.roll(eight, 8, 0)
        lane = lax.broadcasted_iota(jnp.int32, (BLOCK, 128), 1)
        wide = c == 1
        left = jnp.where(wide ^ (x < 0), eight, two)[RIM:]
        right = jnp.where(wide ^ (x < 0), sixteen, four)[RIM:]
        total = jnp.where(lane < 64, left, right)
        base = jnp.where(wide, 8.0, 2.0)
        window = jnp.where(lane < 64, base, base * 2.0)
        count = (lax.broadcasted_iota(jnp.int32, (BLOCK, 128), 0) + (z * BLOCK + 1)).astype(F32)
        mean = (total / jnp.minimum(count, window) - values[RIM:]).astype(BF)
        zero = jnp.zeros((64, 64), F32)
        w0 = jnp.concatenate([pwv[0].astype(F32), zero], axis=1)
        w1 = jnp.concatenate([zero, pwv[1].astype(F32)], axis=1)
        copies[14].wait()
        copies[16].wait()
        pooled = dot(mean, jnp.concatenate([w0, w1], axis=0).astype(BF)) * ps[...]
        ssq[p] = spread(sumsq(pooled), 4)
        px[c] = (pooled * pg[...]).astype(BF)
        send(px.at[c], px.at[c], psnd.at[0], prcv.at[0], at(z, x, o))

    def pool_rows(t, h):
        rows = pl.ds(pl.multiple_of(t * 128, 128), 128)
        both = jnp.concatenate([px[0, rows], px[1, rows]], axis=1)
        return dot(both, w2[1, :, h * 512 : (h + 1) * 512])

    def far_pool():
        got(px.at[o], psnd.at[0], prcv.at[0])
        for i in (0, 1):
            copies[9 + i].wait()
        got(w2.at[:, pl.ds(pl.multiple_of(o * 128, 128), 128)], wsnd.at[0], wrcv.at[0])
        for h in (0, 1):
            fpool[h] = pool_rows(xf, h).astype(BF)

    def send_far_pool(i):
        rows = pl.ds(pl.multiple_of(i * 32, 32), 32)
        for h, xx in ((0, xr), (1, xl)):
            send(fpool.at[h, rows], fgot.at[h, rows], fsnd.at[0], frcv.at[h], at(z, xx, c))

    own_block = xt.at[z]

    def piece_up(s, k):
        return xt.at[zmod(z - s), xmod(x - k)]

    def piece_down(s, k):
        return xt.at[zmod(z + s), xmod(x + k)]

    def from_below(s):
        return z - s >= 0

    def from_above(s):
        return z + s >= NS

    def side_left(s):
        pair = piece_up(s, 0)

        @pl.when(s >= 3)
        def _():
            sent(own, ysnd.at[0, lax.rem(s, 2)], yrcv.at[0, 0])

        send(pair, pair, ysnd.at[0, lax.rem(s, 2)], yrcv.at[0, s - 1], at(z, xl, 1))

    def side_right(s):
        pair = piece_down(s, 0)

        @pl.when((s >= 3) & from_above(s - 2))
        def _():
            sent(own, ysnd.at[1, lax.rem(s, 2)], yrcv.at[1, 0])

        send(pair, pair, ysnd.at[1, lax.rem(s, 2)], yrcv.at[1, s - 1], at(z, xr, 1))

    def slot(s, k):
        n = 3 * s - 3 + k

        def slots(*numbers):
            def run(work):
                here = [s == v // 3 + 1 for v in numbers if v % 3 == k]
                if here:
                    pl.when(functools.reduce(jnp.logical_or, here))(work)

            return run


        @pl.when(ring_core & from_below(s) & (s < 9))
        def _():
            pair = piece_up(s, k)
            got(pair, usnd.at[0], urcv.at[s - 1, k])

            if k == 0:

                @pl.when((s >= 2) & goes_up(s - 2) & (s < 8))
                def _():
                    sent(xt.at[z, 0:3], usnd.at[lax.rem(s, 2)], urcv.at[0, 0])

            @pl.when((s < 8) & (z < NS - 1))
            def _():
                up(s, k, pair)

            if k == 0:

                @pl.when(s >= 3)
                def _():
                    side_left(s)

        @pl.when(ring_core & goes_down(s) & (s < 8))
        def _():
            pair = piece_down(s, k)
            got(pair, dsnd.at[0], drcv.at[s - 1, k])

            @pl.when(s < 7)
            def _():
                if k == 0:

                    @pl.when((s >= 2) & goes_down(s - 2))
                    def _():
                        sent(xt.at[z, 0:3], dsnd.at[lax.rem(s, 2)], drcv.at[0, 0])

                down(s, k, pair)

            if k == 0:

                @pl.when((s >= 3) & from_above(s))
                def _():
                    side_right(s)

        @slots(0)
        def _():
            @pl.when(ring_core)
            def _():
                send(piece, piece, nsnd.at[0], orcv.at[15], at(z, x, 0))
                for i, xx in enumerate((xr, xl, xf)):
                    pair = xt.at[z, xx]
                    send(pair, pair, nsnd.at[0], orcv.at[16 + i], at(z, x, 0))

        @slots(4, 5)
        def _():
            @pl.when(ring_core)
            def _():
                @pl.when(from_below(n - 3))
                def _():
                    side_left(n - 3)

                @pl.when(from_above(n - 3))
                def _():
                    side_right(n - 3)

        @slots(8)
        def _():
            @pl.when(ring_core)
            def _():
                sides(1)
                sides(2)

        if k == 1:

            @pl.when(ring_core & (s >= 4))
            def _():
                sides(s - 1)

        @slots(0)
        def _():
            @pl.when(rows_core)
            def _():
                got(trows(xl, 0), tsnd.at[0], trcv.at[0, 0])
                right(0, 2, xl)
                got(trows(xr, 1), tsnd.at[0], trcv.at[1, 1])
                left(1, 2, xr)

        @slots(3)
        def _():
            @pl.when(rows_core)
            def _():
                got(xt.at[z, x, 1], nsnd.at[0], orcv.at[15])
                for i, xx in enumerate((xr, xl, xf)):
                    got(xt.at[z, xx], nsnd.at[0], orcv.at[16 + i])

            expand(z)

        def pass_on(i, xx):
            block = nt.at[pl.ds(xx * 2, 2)]
            send(block, block, vsnd.at[0], vrcv.at[i], at(z, x, 1))

        def passed(i, xx):
            got(nt.at[pl.ds(xx * 2, 2)], vsnd.at[0], vrcv.at[i])

        @slots(4)
        def _():
            @pl.when(rows_core)
            def _():
                got(trows(xl, 1), tsnd.at[0], trcv.at[0, 1])
                pass_on(1, xl)
                got(trows(xr, 0), tsnd.at[0], trcv.at[1, 0])
                pass_on(2, xr)

        @slots(6)
        def _():
            copies[4].wait()

            @pl.when(ring_core)
            def _():
                got(trows(x, 0), vsnd.at[0], vrcv.at[0])
                passed(1, xl)
                passed(2, xr)

            project((x, xl, xr))

        @slots(7)
        def _():
            @pl.when(rows_core)
            def _():
                got(trows(xf, 0), tsnd.at[0], trcv.at[0, 2])
                got(trows(xf, 1), tsnd.at[0], trcv.at[1, 2])
                pass_on(3, xf)

        @slots(10)
        def _():
            @pl.when(ring_core)
            def _():
                passed(3, xf)

            project((xf,))
            rim[...] = poolin[BLOCK:, :].astype(BF)

            @pl.when(z < NS - 1)
            def _():
                send(rim, halo, hsnd.at[0], hrcv.at[0], at(zu, x, c))

        @slots(START)
        def _():
            attend(z, True)

        @slots(START + 2)
        def _():
            copies[7].wait()
            pool()

        @slots(16)
        def _():
            far_pool()

        @slots(16, 17, 19, 20)
        def _():
            send_far_pool(jnp.where(n < 18, n - 16, n - 17))

        e = jnp.where(n < 26, n - 10, 15)
        je = block_of(e)
        due = (n >= 11) & (n != 25) & (je >= 0)
        ja = block_of(n - 11)
        ripe = (n >= 12) & (n <= 25) & (ja >= 0)

        @pl.when(due & rows_core)
        def _():
            got(xt.at[je], nsnd.at[0], orcv.at[e - 1])

        @pl.when(due & ripe)
        def _():
            attend(ja, False)
            expand(je)

        @pl.when(due != ripe)
        def _():
            @pl.when(due)
            def _():
                expand(je)

            @pl.when(ripe)
            def _():
                attend(ja, False)

    def step(s, carry):
        for k in range(3):
            slot(s, k)
        return carry

    def sides(s):
        @pl.when(from_below(s))
        def _():
            pair = xt.at[zmod(z - s), xr]
            got(pair, ysnd.at[0, 0], yrcv.at[0, s - 1])
            ssem = osnd.at[0, lax.rem(s, 2)]

            @pl.when(s >= 3)
            def _():
                sent(own_block, ssem, orcv.at[15])

            other(ssem, 2 * s - 2, zmod(z - s))

        @pl.when(from_above(s) & (s < 8))
        def _():
            pair = xt.at[zmod(z + s), xl]
            got(pair, ysnd.at[1, 0], yrcv.at[1, s - 1])
            ssem = osnd.at[1, lax.rem(s, 2)]

            @pl.when((s >= 3) & from_above(s - 2))
            def _():
                sent(own_block, ssem, orcv.at[15])

            other(ssem, 2 * s - 1, zmod(z + s))

    lax.fori_loop(1, 10, step, 0)

    @pl.when(z >= 8)
    def _():
        attend(z - 8, False)

    copies[15].wait()
    attended = acc[:, :128] / acc[:, 128:]
    ax[c] = (attended * ag[...]).astype(BF)
    send(ax.at[c], ax.at[c], psnd.at[1], prcv.at[1], at(z, x, o))
    ssq[p] = ssq[p] + spread(sumsq(attended), 0)
    for xx, cc in [(xf, c), (xf, o), (xr, c), (xl, c), (xr, o), (xl, o), (x, o)]:
        send(ssq.at[p], ssq.at[p], ssnd.at[0], srcv.at[0], at(z, xx, cc))
    for t in (xr, xl, x):
        for h in (0, 1):
            bpart[t, h] = pool_rows(t, h)

    def mixed_rows(t, h):
        rows = pl.ds(pl.multiple_of(t * 128, 128), 128)
        both = jnp.concatenate([ax[0, rows], ax[1, rows]], axis=1)
        return dot(both, w2[0, :, h * 512 : (h + 1) * 512])

    got(ax.at[o], psnd.at[1], prcv.at[1])
    for h in (0, 1):
        part[xf, h] = mixed_rows(xf, h).astype(BF)
    send(part.at[xf, 0], far.at[0], rsnd.at[0], rrcv.at[0], at(z, xr, c))
    send(part.at[xf, 1], far.at[1], rsnd.at[0], rrcv.at[1], at(z, xl, c))
    got(ssq.at[0:7], ssnd.at[0], srcv.at[0])
    total = ssq[0]
    for i in range(1, 8):
        total = total + ssq[i]
    factor = lax.rsqrt(total * (1.0 / 1024.0) + EPS)
    fcol[...] = jnp.concatenate([factor, jnp.zeros((120, 128), F32)], axis=0).T

    lane = lax.broadcasted_iota(jnp.int32, (128, 128), 1)

    def pick(k):
        return jnp.sum(jnp.where(lane == k, fcol[...], 0.0), axis=1, keepdims=True)

    def partial(t, hs):
        fa, fp = pick(t), pick(t + 4)
        for h in hs:
            part[t, h] = (mixed_rows(t, h) * fa + bpart[t, h] * fp).astype(BF)

    def combined(t, h):
        term = mixed_rows(t, h) + far[h].astype(F32)
        base = bpart[t, h] + fgot[h].astype(F32)
        part[t, h] = (term * pick(t) + base * pick(t + 4)).astype(BF)

    def rrows(cc):
        return pl.ds(pl.multiple_of(cc * ROWS, ROWS), ROWS)

    def to_right(h, i):
        for cc in (0, 1):
            send(part.at[xr, h, rrows(cc)], fin.at[c, i], esnd.at[0], ercv.at[0], at(z, xr, cc))

    def to_left(h, i):
        for cc in (0, 1):
            send(part.at[xl, h, rrows(cc)], fin.at[c, i], esnd.at[0], ercv.at[0], at(z, xl, cc))

    partial(xr, (1,))
    to_right(1, 2)
    partial(xl, (0,))
    to_left(0, 0)
    partial(x, (0, 1))
    send(part.at[x, :, rrows(o)], ownp, rsnd.at[1], rrcv.at[2], at(z, x, o))
    for i in (0, 1):
        got(fgot.at[i], fsnd.at[0], frcv.at[i])
    got(far.at[0], rsnd.at[0], rrcv.at[0])
    combined(xr, 0)
    to_right(0, 1)
    got(far.at[1], rsnd.at[0], rrcv.at[1])
    combined(xl, 1)
    to_left(1, 3)

    got(ownp, rsnd.at[1], rrcv.at[2])
    got(fin, esnd.at[0], ercv.at[0])
    for h in (0, 1):
        for sub in (0, 1):
            mixed = fin[h, 2 * sub].astype(F32) + fin[h, 2 * sub + 1].astype(F32)
            here = jnp.where(c == h, part[x, sub, rrows(c)].astype(F32), ownp[sub].astype(F32))
            lo = h * 1024 + sub * 512
            out[0, :, lo : lo + 512] = (mixed + here).astype(BF)

    @pl.when(rows_core)
    def _():
        sent(xt.at[z, 0:2], gsnd.at[0], grcv.at[0, 0])
        sent(nt.at[0:6], tsnd.at[0], trcv.at[0, 0])
        sent(nt.at[0:7], vsnd.at[0], vrcv.at[0])

    @pl.when(ring_core)
    def _():
        sent(xt.at[z, 0:3, 0], gsnd.at[0], grcv.at[0, 0])
        sent(nt.at[p], vsnd.at[0], vrcv.at[0])
        sent(xt.at[0:7, 0, 0], nsnd.at[0], orcv.at[15])

    sent(w2.at[:, wrows], wsnd.at[0], wrcv.at[0])
    for i in (0, 1):
        sent(px.at[c], psnd.at[i], prcv.at[i])
    sent(far, rsnd.at[0], rrcv.at[0])
    sent(ownp, rsnd.at[1], rrcv.at[2])
    sent(fpool, fsnd.at[0], frcv.at[0])
    sent(ssq.at[0:7], ssnd.at[0], srcv.at[0])
    sent(fin, esnd.at[0], ercv.at[0])

    @pl.when(z < NS - 1)
    def _():
        sent(rim, hsnd.at[0], hrcv.at[0])

    def drain(s, carry):
        odd = lax.rem(s, 2)
        other_odd = 1 - odd

        @pl.when(goes_up(s) & jnp.logical_not(goes_up(s + 2) & (s < 6)))
        def _():
            sent(xt.at[z, 0:3], usnd.at[odd], urcv.at[0, 0])

        @pl.when(goes_down(s) & (s < 7) & jnp.logical_not(goes_down(s + 2) & (s < 5)))
        def _():
            sent(xt.at[z, 0:3], dsnd.at[odd], drcv.at[0, 0])

        @pl.when(from_below(s + 1) & jnp.logical_not(from_below(s + 3) & (s < 6)))
        def _():
            sent(own, ysnd.at[0, other_odd], yrcv.at[0, 0])
            sent(own_block, osnd.at[0, other_odd], orcv.at[15])

        @pl.when(from_above(s + 1) & (s < 7) & jnp.logical_not(from_above(s + 3) & (s < 5)))
        def _():
            sent(own, ysnd.at[1, other_odd], yrcv.at[1, 0])
            sent(own_block, osnd.at[1, other_odd], orcv.at[15])

        return carry

    @pl.when(ring_core)
    def _():
        lax.fori_loop(0, 8, drain, 0)


def rope_table(length):
    halfway = 16
    inv = (1.0 / np.float32(THETA) ** (np.arange(halfway, dtype=np.float32) / np.float32(halfway))).astype(np.float32)
    angle = (np.arange(length, dtype=np.float32)[None, :] * inv[:, None]).astype(np.float32).astype(np.float64)
    return np.concatenate([np.cos(angle), np.sin(angle)], axis=0).astype(np.float32)


def local(
    tokens, input_gain, query_weight, latent_down, rotary_down, pool_down, key_up, value_up,
    query_gain, key_gain, pool_weight, pool_scale, attention_gain, pool_gain, attention_out, pool_out,
):
    width = tokens.shape[2]
    table = jnp.asarray(rope_table(NS * BLOCK))
    hbm = pl.BlockSpec(memory_space=pl.ANY)
    vmem = pl.BlockSpec(memory_space=pltpu.VMEM)
    V = pltpu.VMEM
    D = pltpu.SemaphoreType.DMA
    half = width // 2
    scratch = [
        V((ROWS, width), BF), V((1, width), F32), V((8, ROWS, width), BF), V((QK, width), BF),
        V((width, 256), BF), V((32, width), BF), V((width, 256), BF), V((256, 128), BF), V((256, 128), BF),
        V((1, QK), F32), V((1, QK), F32), V((2, 64, 64), BF), V((1, 128), F32), V((1, 128), F32),
        V((1, 128), F32), V((2, 256, half), BF), V((32, NS * BLOCK), F32),
        V((NS, NX, 2, 144, 128), BF), V((128, 256), BF), V((128, 256), BF), V((BLOCK, 128), BF),
        V((NS, 128, BLOCK), BF), V((NS, 128, BLOCK), BF), V((BLOCK, 256), F32),
        V((QK, 128), F32), V((QK, 128), F32),
        V((RIM, 128), BF), V((RIM, 128), BF), V((BLOCK + RIM, 128), F32), V((2, BLOCK, 128), BF),
        V((2, BLOCK, 128), BF), V((NX, 2, 128, half // 2), F32),
        V((8, 8, 128), F32), V((NX, 2, 128, half // 2), BF), V((2, 128, half // 2), BF),
        V((2, 4, ROWS, half // 2), BF), V((2, ROWS, half // 2), BF), V((128, 128), F32), V((2, 128, half // 2), BF), V((2, 128, half // 2), BF),
        D((17,)),
        D((2,)), D((8, 3)), D((2,)), D((7, 3)), D((2, 2)), D((2, 8)), D((1,)), D((4, 2)),
        D((2, 2)), D((19,)), D((1,)), D((2,)), D((2,)),
        D((1,)), D((2, 3)), D((1,)), D((4,)), D((1,)), D((1,)), D((1,)), D((1,)),
        D((1,)), D((1,)), D((1,)), D((1,)), D((2,)), D((3,)), D((1,)), D((2,)),
    ]
    args = (
        tokens, input_gain.reshape(1, -1), query_weight.T, latent_down, rotary_down.T, pool_down, key_up, value_up,
        query_gain.reshape(1, -1), key_gain.reshape(1, -1), pool_weight, pool_scale.reshape(1, -1),
        attention_gain.reshape(1, -1), pool_gain.reshape(1, -1), attention_out, pool_out, table,
    )
    specs = [hbm] * 17
    return pl.pallas_call(
        kernel,
        out_shape=pltpu.VMEM(tokens.shape, BF),
        in_specs=specs,
        out_specs=vmem,
        scratch_shapes=scratch,
        compiler_params=pltpu.CompilerParams(
            collective_id=0, has_side_effects=True, vmem_limit_bytes=60 * 1024 * 1024
        ),
    )(*args)


def solution(mesh):
    placed = (
        P("fs", ("sp", "tp"), None), P(), P(None, "tp"), P(), P(), P(None, "tp"), P(), P(),
        P(), P(), P(), P("tp"), P("tp"), P("tp"), P("tp", None), P("tp", None),
    )
    return jax.shard_map(
        local, mesh=mesh, in_specs=placed, out_specs=P("fs", ("sp", "tp"), None), check_vma=False
    )
```

```python
import functools
import math

import jax
import jax.numpy as jnp
import numpy as np
from jax import lax
from jax.experimental import pallas as pl
from jax.experimental.pallas import tpu as pltpu
from jax.sharding import PartitionSpec as P

MESH = pl.DeviceIdType.MESH
BF = jnp.bfloat16
F32 = jnp.float32

EPS = 1e-06
THETA = 10000.0
QK = 96
SCALE = math.log2(math.e) / math.sqrt(QK)
NX = 4
NS = 16
BLOCK = 512
ROWS = 64
RIM = 16
START = 11


def dot(a, b, dims=((1,), (0,)), precision=None):
    return lax.dot_general(a, b, (dims, ((), ())), preferred_element_type=F32, precision=precision)


def kernel(
    tokens, igh, qw, ld, rd, pd, ku, vu, qgh, kgh, pw, psh, agh, pgh, ao, po, tab,
    out,
    tokv, ig, nt, qwv, ldv, rdv, wv, kuv, vuv, qg, kg, pwv, ps, ag, pg, w2, tabv,
    xt, kut, vut, qv, ktv, vtv, acc, qcol, kcol, rim, halo, poolin, px, ax, bpart,
    ssq, part, far, fin, ownp, fcol, fpool, fgot,
    dsem, usnd, urcv, dsnd, drcv, ysnd, yrcv, gsnd, grcv, osnd, orcv, nsnd, psnd, prcv,
    tsnd, trcv, vsnd, vrcv, wsnd, wrcv, hsnd, hrcv, esnd, ercv, ssnd, srcv, rsnd, rrcv, fsnd, frcv,
):
    z = lax.axis_index("sp")
    fs = lax.axis_index("fs")
    p = lax.axis_index("tp")
    c = lax.rem(p, 2)
    x = p // 2
    o = 1 - c

    def zmod(v):
        return lax.rem(v + 2 * NS, NS)

    def xmod(v):
        return lax.rem(v + 2 * NX, NX)

    def at(zz, xx, cc):
        return (zz, fs, xx * 2 + cc)

    xr, xl, xf = xmod(x + 1), xmod(x - 1), xmod(x + 2)
    zu, zd = zmod(z + 1), zmod(z - 1)

    def send(src, dst, ssem, rsem, dev):
        copy = pltpu.make_async_remote_copy(
            src_ref=src, dst_ref=dst, send_sem=ssem, recv_sem=rsem, device_id=dev, device_id_type=MESH
        )
        copy.start()

    def got(dst, ssem, rsem):
        pltpu.make_async_remote_copy(
            src_ref=dst, dst_ref=dst, send_sem=ssem, recv_sem=rsem,
            device_id=at(z, x, o), device_id_type=MESH,
        ).wait_recv()

    def sent(src, ssem, rsem):
        pltpu.make_async_remote_copy(
            src_ref=src, dst_ref=src, send_sem=ssem, recv_sem=rsem,
            device_id=at(z, x, o), device_id_type=MESH,
        ).wait_send()

    barrier = pltpu.get_barrier_semaphore()
    peers = [at(z, x, o), at(zu, x, c), at(zd, x, c)]
    peers += [at(z, xx, cc) for xx in (xr, xl, xf) for cc in (c, o)]
    for peer in peers:
        pl.semaphore_signal(barrier, inc=1, device_id=peer, device_id_type=MESH)

    half = out.shape[2] // 2
    mine = pl.ds(pl.multiple_of(c * half, 128), half)
    theirs = pl.ds(pl.multiple_of(o * half, 128), half)
    kcols = pl.ds(pl.multiple_of(x * 128, 128), 128)
    vcols = pl.ds(pl.multiple_of(p * 128, 128), 128)
    wrows = pl.ds(pl.multiple_of(c * 128, 128), 128)
    loads = [
        (tokens.at[0], tokv),
        (ld, ldv),
        (rd, rdv),
        (qw, qwv),
        (pd, wv.at[:, 0:128]),
        (ku.at[:, kcols], kuv),
        (vu.at[:, vcols], vuv),
        (pw.at[pl.ds(p * 2, 2)], pwv),
        (tab, tabv),
        (ao.at[:, mine], w2.at[0, wrows]),
        (po.at[:, mine], w2.at[1, wrows]),
        (igh, ig),
        (qgh, qg),
        (kgh, kg),
        (psh, ps),
        (agh, ag),
        (pgh, pg),
    ]
    copies = [pltpu.make_async_copy(s, d, dsem.at[i]) for i, (s, d) in enumerate(loads)]
    for i in (0, 11, 1, 2, 5, 6, 12, 13, 3, 4, 8, 7, 9, 10, 14, 15, 16):
        copies[i].start()

    copies[0].wait()
    copies[11].wait()
    source = tokv[...].astype(F32)
    scale = lax.rsqrt(jnp.mean(source * source, axis=1, keepdims=True) + EPS)
    normed = (source * scale * ig[...]).astype(BF)
    nt[p] = normed
    copies[1].wait()
    copies[2].wait()
    latent = dot(normed, ldv[...]).astype(BF).astype(F32)
    rotary = dot(rdv[...], normed, ((1,), (1,))).astype(BF).astype(F32)
    swap = (lax.broadcasted_iota(jnp.int32, (16, ROWS), 0) + c * 16) >= 16
    turned = [jnp.where(swap, rotary[16:32], rotary[:16]), jnp.where(swap, rotary[:16], rotary[16:32])]
    lat = latent * lax.rsqrt(jnp.mean(latent * latent, axis=1, keepdims=True) + EPS)
    swap = (lax.broadcasted_iota(jnp.int32, (ROWS, 128), 0) + c * 2 * ROWS) >= 2 * ROWS
    stacked = jnp.concatenate(
        [jnp.where(swap, lat[:, 128:], lat[:, :128]), jnp.where(swap, lat[:, :128], lat[:, 128:])], axis=0
    )
    xt[z, x, c, 0:128, :] = stacked.T.astype(BF)
    xt[z, x, c, 128:144, :] = jnp.concatenate(turned, axis=1).astype(BF)

    pl.semaphore_wait(barrier, len(peers))

    rows_core, ring_core = c == 0, c == 1
    own = xt.at[z, x]
    piece = xt.at[z, x, c]

    def up(s, k, pair):
        send(pair, pair, usnd.at[lax.rem(s, 2)], urcv.at[s, k], at(zu, x, 1))

    def down(s, k, pair):
        send(pair, pair, dsnd.at[lax.rem(s, 2)], drcv.at[s, k], at(zd, x, 1))

    def other(ssem, sem, j):
        send(xt.at[j], xt.at[j], ssem, orcv.at[sem], at(z, x, 0))

    def goes_up(s):
        return (z - s >= 0) & (z < NS - 1)

    def goes_down(s):
        return (z + s <= 6) | (z + s >= NS)

    @pl.when(rows_core)
    def _():
        send(piece, piece, gsnd.at[0], grcv.at[0, 0], at(z, x, 1))

    send(piece, piece, gsnd.at[0], grcv.at[3, c], at(z, xr, 1))
    send(piece, piece, gsnd.at[0], grcv.at[1, c], at(z, xl, 1))
    send(piece, piece, gsnd.at[0], grcv.at[2, c], at(z, xf, 1))

    def trows(xx, h):
        return nt.at[xx * 2 + h]

    def right(h, i, xx):
        send(trows(xx, h), trows(xx, h), tsnd.at[0], trcv.at[0, i], at(z, xr, 0))

    def left(h, i, xx):
        send(trows(xx, h), trows(xx, h), tsnd.at[0], trcv.at[1, i], at(z, xl, 0))

    send(nt.at[p], nt.at[p], vsnd.at[0], vrcv.at[0], at(z, x, o))

    @pl.when(rows_core)
    def _():
        right(0, 0, x)
        got(trows(x, 1), vsnd.at[0], vrcv.at[0])
        left(1, 1, x)
        right(1, 1, x)
        left(0, 0, x)

    @pl.when(ring_core)
    def _():
        got(piece, gsnd.at[0], grcv.at[0, 0])

        @pl.when(goes_up(0))
        def _():
            up(0, 0, own)

        @pl.when(goes_down(0))
        def _():
            down(0, 0, own)

    for i, w in enumerate((ao, po)):
        send(w.at[:, theirs], w2.at[i, wrows], wsnd.at[0], wrcv.at[0], at(z, x, o))

    copies[5].wait()
    copies[6].wait()
    kut[...] = kuv[...].astype(F32).T.astype(BF)
    vut[...] = vuv[...].astype(F32).T.astype(BF)
    copies[12].wait()
    copies[13].wait()
    qcol[...] = jnp.broadcast_to(qg[...], (128, QK)).T
    kcol[...] = jnp.broadcast_to(kg[...], (128, QK)).T
    acc[...] = jnp.zeros_like(acc)
    copies[3].wait()
    for i in range(qwv.shape[1] // 128):
        cols = slice(i * 128, (i + 1) * 128)
        tile = jnp.concatenate([qwv[:, cols].astype(F32), jnp.zeros((128 - QK, 128), F32)], axis=0)
        wv[cols, 128:256] = tile.T.astype(BF)

    def gathered(rel):
        pair = xt.at[z, xmod(x + rel)]
        for i in (0, 1):
            got(piece, gsnd.at[0], grcv.at[rel, i])
        if rel != 1:

            @pl.when(goes_up(0))
            def _():
                up(0, 4 - rel, pair)

        if rel != 3:

            @pl.when(goes_down(0))
            def _():
                down(0, rel, pair)

    @pl.when(ring_core)
    def _():
        gathered(1)
        gathered(3)
        gathered(2)

    copies[8].wait()

    def rotate(a, b, first):
        cosine = tabv[0:16, pl.ds(first, a.shape[1])]
        sine = tabv[16:32, pl.ds(first, a.shape[1])]
        return a * cosine - b * sine, b * cosine + a * sine

    def expand(j):
        lane = lax.broadcasted_iota(jnp.int32, (144, 128), 1)
        low, high = [], []
        for xx in range(NX):
            p0 = xt[j, xx, 0].astype(F32)
            p1 = xt[j, xx, 1].astype(F32)
            low.append(jnp.where(lane < 64, p0, p1))
            high.append(pltpu.roll(jnp.where(lane < 64, p1, p0), 64, 1))
        low = jnp.concatenate(low, axis=1)
        high = jnp.concatenate(high, axis=1)
        lat2 = jnp.concatenate([low[:128].astype(BF), high[:128].astype(BF)], axis=0)
        plain = dot(kut[pl.ds(pl.multiple_of(c * 64, 64), 64), :], lat2)
        vtv[j] = dot(vut[...], lat2).astype(BF)
        a, b = low[128:144], high[128:144]
        total = jnp.sum(plain * plain, axis=0, keepdims=True)
        total = total + jnp.sum(a * a + b * b, axis=0, keepdims=True)
        factor = lax.rsqrt(total * (1.0 / QK) + EPS)
        gain = kcol[:, 0:1]
        first = pl.multiple_of(j * BLOCK, 128)
        a, b = rotate(a * factor * gain[64:80], b * factor * gain[80:96], first)
        ktv[j, 0:64, :] = (plain * factor * gain[0:64]).astype(BF)
        ktv[j, 64:80, :] = a.astype(BF)
        ktv[j, 80:96, :] = b.astype(BF)
        ktv[j, QK:128, :] = jnp.zeros((128 - QK, BLOCK), BF)

    def attend(j, masked):
        both = jnp.concatenate([vtv[j], jnp.ones((128, BLOCK), BF)], axis=0)
        weight = jnp.exp2(dot(qv[...], ktv[j]))
        if masked:
            qpos = lax.broadcasted_iota(jnp.int32, weight.shape, 0)
            kpos = lax.broadcasted_iota(jnp.int32, weight.shape, 1)
            weight = jnp.where(kpos <= qpos, weight, 0.0)
        acc[...] += dot(weight.astype(BF), both, ((1,), (1,)))

    def block_of(u):
        return jnp.where(lax.rem(u, 2) == 1, z - (u + 1) // 2, z + u // 2 - NS)

    def project(chips):
        rows = [nt[2 * t + i] for t in chips for i in (0, 1)]
        both = dot(jnp.concatenate(rows, axis=0), wv[...])
        raws = both[:, 128:].T[:QK]
        for i, t in enumerate(chips):
            spot = pl.ds(pl.multiple_of(t * 128, 128), 128)
            poolin[pl.ds(pl.multiple_of(t * 128 + RIM, 8), 128), :] = (
                both[i * 128 : (i + 1) * 128, :128].astype(BF).astype(F32)
            )
            raw = raws[:, i * 128 : (i + 1) * 128]
            total = jnp.sum(raw * raw, axis=0, keepdims=True)
            normal = raw * lax.rsqrt(total * (1.0 / QK) + EPS) * qcol[:, 0:1] * SCALE
            first = pl.multiple_of(z * BLOCK + t * 128, 128)
            a, b = rotate(normal[64:80], normal[80:96], first)
            full = jnp.concatenate([normal[:64], a, b, jnp.zeros((32, 128), F32)], axis=0)
            qv[spot, :] = full.T.astype(BF)

    def sumsq(values):
        total = jnp.sum((values * values).T, axis=0, keepdims=True)
        return jnp.broadcast_to(total, (8, BLOCK))

    def spread(totals, start):
        sub = lax.broadcasted_iota(jnp.int32, (8, 128), 0)
        packed = jnp.zeros((8, 128), F32)
        for t in range(NX):
            packed = jnp.where(sub == start + t, totals[:, t * 128 : (t + 1) * 128], packed)
        return packed

    def pool():
        @pl.when(z > 0)
        def _():
            got(halo, hsnd.at[0], hrcv.at[0])

        poolin[0:RIM, :] = jnp.where(z > 0, halo[...].astype(F32), 0.0)
        values = poolin[...]
        two = values + pltpu.roll(values, 1, 0)
        four = two + pltpu.roll(two, 2, 0)
        eight = four + pltpu.roll(four, 4, 0)
        sixteen = eight + pltpu.roll(eight, 8, 0)
        lane = lax.broadcasted_iota(jnp.int32, (BLOCK, 128), 1)
        wide = c == 1
        left = jnp.where(wide ^ (x < 0), eight, two)[RIM:]
        right = jnp.where(wide ^ (x < 0), sixteen, four)[RIM:]
        total = jnp.where(lane < 64, left, right)
        base = jnp.where(wide, 8.0, 2.0)
        window = jnp.where(lane < 64, base, base * 2.0)
        count = (lax.broadcasted_iota(jnp.int32, (BLOCK, 128), 0) + (z * BLOCK + 1)).astype(F32)
        mean = (total / jnp.minimum(count, window) - values[RIM:]).astype(BF)
        zero = jnp.zeros((64, 64), F32)
        w0 = jnp.concatenate([pwv[0].astype(F32), zero], axis=1)
        w1 = jnp.concatenate([zero, pwv[1].astype(F32)], axis=1)
        copies[14].wait()
        copies[16].wait()
        pooled = dot(mean, jnp.concatenate([w0, w1], axis=0).astype(BF)) * ps[...]
        ssq[p] = spread(sumsq(pooled), 4)
        px[c] = (pooled * pg[...]).astype(BF)
        send(px.at[c], px.at[c], psnd.at[0], prcv.at[0], at(z, x, o))

    def pool_rows(t, h):
        rows = pl.ds(pl.multiple_of(t * 128, 128), 128)
        both = jnp.concatenate([px[0, rows], px[1, rows]], axis=1)
        return dot(both, w2[1, :, h * 512 : (h + 1) * 512])

    def far_pool():
        got(px.at[o], psnd.at[0], prcv.at[0])
        for i in (0, 1):
            copies[9 + i].wait()
        got(w2.at[:, pl.ds(pl.multiple_of(o * 128, 128), 128)], wsnd.at[0], wrcv.at[0])
        for h in (0, 1):
            fpool[h] = pool_rows(xf, h).astype(BF)

    def send_far_pool(i):
        rows = pl.ds(pl.multiple_of(i * 32, 32), 32)
        for h, xx in ((0, xr), (1, xl)):
            send(fpool.at[h, rows], fgot.at[h, rows], fsnd.at[0], frcv.at[h], at(z, xx, c))

    own_block = xt.at[z]

    def piece_up(s, k):
        return xt.at[zmod(z - s), xmod(x - k)]

    def piece_down(s, k):
        return xt.at[zmod(z + s), xmod(x + k)]

    def from_below(s):
        return z - s >= 0

    def from_above(s):
        return z + s >= NS

    def side_left(s):
        pair = piece_up(s, 0)

        @pl.when(s >= 3)
        def _():
            sent(own, ysnd.at[0, lax.rem(s, 2)], yrcv.at[0, 0])

        send(pair, pair, ysnd.at[0, lax.rem(s, 2)], yrcv.at[0, s - 1], at(z, xl, 1))

    def side_right(s):
        pair = piece_down(s, 0)

        @pl.when((s >= 3) & from_above(s - 2))
        def _():
            sent(own, ysnd.at[1, lax.rem(s, 2)], yrcv.at[1, 0])

        send(pair, pair, ysnd.at[1, lax.rem(s, 2)], yrcv.at[1, s - 1], at(z, xr, 1))

    def slot(s, k):
        n = 3 * s - 3 + k

        def slots(*numbers):
            def run(work):
                here = [s == v // 3 + 1 for v in numbers if v % 3 == k]
                if here:
                    pl.when(functools.reduce(jnp.logical_or, here))(work)

            return run


        @pl.when(ring_core & from_below(s) & (s < 9))
        def _():
            pair = piece_up(s, k)
            got(pair, usnd.at[0], urcv.at[s - 1, k])

            if k == 0:

                @pl.when((s >= 2) & goes_up(s - 2) & (s < 8))
                def _():
                    sent(xt.at[z, 0:3], usnd.at[lax.rem(s, 2)], urcv.at[0, 0])

            @pl.when((s < 8) & (z < NS - 1))
            def _():
                up(s, k, pair)

            if k == 0:

                @pl.when(s >= 3)
                def _():
                    side_left(s)

        @pl.when(ring_core & goes_down(s) & (s < 8))
        def _():
            pair = piece_down(s, k)
            got(pair, dsnd.at[0], drcv.at[s - 1, k])

            @pl.when(s < 7)
            def _():
                if k == 0:

                    @pl.when((s >= 2) & goes_down(s - 2))
                    def _():
                        sent(xt.at[z, 0:3], dsnd.at[lax.rem(s, 2)], drcv.at[0, 0])

                down(s, k, pair)

            if k == 0:

                @pl.when((s >= 3) & from_above(s))
                def _():
                    side_right(s)

        @slots(0)
        def _():
            @pl.when(ring_core)
            def _():
                send(piece, piece, nsnd.at[0], orcv.at[15], at(z, x, 0))
                for i, xx in enumerate((xr, xl, xf)):
                    pair = xt.at[z, xx]
                    send(pair, pair, nsnd.at[0], orcv.at[16 + i], at(z, x, 0))

        @slots(4, 5)
        def _():
            @pl.when(ring_core)
            def _():
                @pl.when(from_below(n - 3))
                def _():
                    side_left(n - 3)

                @pl.when(from_above(n - 3))
                def _():
                    side_right(n - 3)

        @slots(8)
        def _():
            @pl.when(ring_core)
            def _():
                sides(1)
                sides(2)

        if k == 1:

            @pl.when(ring_core & (s >= 4))
            def _():
                sides(s - 1)

        @slots(0)
        def _():
            @pl.when(rows_core)
            def _():
                got(trows(xl, 0), tsnd.at[0], trcv.at[0, 0])
                right(0, 2, xl)
                got(trows(xr, 1), tsnd.at[0], trcv.at[1, 1])
                left(1, 2, xr)

        @slots(3)
        def _():
            @pl.when(rows_core)
            def _():
                got(xt.at[z, x, 1], nsnd.at[0], orcv.at[15])
                for i, xx in enumerate((xr, xl, xf)):
                    got(xt.at[z, xx], nsnd.at[0], orcv.at[16 + i])

            expand(z)

        def pass_on(i, xx):
            block = nt.at[pl.ds(xx * 2, 2)]
            send(block, block, vsnd.at[0], vrcv.at[i], at(z, x, 1))

        def passed(i, xx):
            got(nt.at[pl.ds(xx * 2, 2)], vsnd.at[0], vrcv.at[i])

        @slots(4)
        def _():
            @pl.when(rows_core)
            def _():
                got(trows(xl, 1), tsnd.at[0], trcv.at[0, 1])
                pass_on(1, xl)
                got(trows(xr, 0), tsnd.at[0], trcv.at[1, 0])
                pass_on(2, xr)

        @slots(6)
        def _():
            copies[4].wait()

            @pl.when(ring_core)
            def _():
                got(trows(x, 0), vsnd.at[0], vrcv.at[0])
                passed(1, xl)
                passed(2, xr)

            project((x, xl, xr))

        @slots(7)
        def _():
            @pl.when(rows_core)
            def _():
                got(trows(xf, 0), tsnd.at[0], trcv.at[0, 2])
                got(trows(xf, 1), tsnd.at[0], trcv.at[1, 2])
                pass_on(3, xf)

        @slots(10)
        def _():
            @pl.when(ring_core)
            def _():
                passed(3, xf)

            project((xf,))
            rim[...] = poolin[BLOCK:, :].astype(BF)

            @pl.when(z < NS - 1)
            def _():
                send(rim, halo, hsnd.at[0], hrcv.at[0], at(zu, x, c))

        @slots(START)
        def _():
            attend(z, True)

        @slots(START + 2)
        def _():
            copies[7].wait()
            pool()

        @slots(16)
        def _():
            far_pool()

        @slots(16, 17, 19, 20)
        def _():
            send_far_pool(jnp.where(n < 18, n - 16, n - 17))

        e = jnp.where(n < 26, n - 10, 15)
        je = block_of(e)
        due = (n >= 11) & (n != 25) & (je >= 0)
        ja = block_of(n - 11)
        ripe = (n >= 12) & (n <= 25) & (ja >= 0)

        @pl.when(due & rows_core)
        def _():
            got(xt.at[je], nsnd.at[0], orcv.at[e - 1])

        @pl.when(due & ripe)
        def _():
            attend(ja, False)
            expand(je)

        @pl.when(due != ripe)
        def _():
            @pl.when(due)
            def _():
                expand(je)

            @pl.when(ripe)
            def _():
                attend(ja, False)

    def step(s, carry):
        for k in range(3):
            slot(s, k)
        return carry

    def sides(s):
        @pl.when(from_below(s))
        def _():
            pair = xt.at[zmod(z - s), xr]
            got(pair, ysnd.at[0, 0], yrcv.at[0, s - 1])
            ssem = osnd.at[0, lax.rem(s, 2)]

            @pl.when(s >= 3)
            def _():
                sent(own_block, ssem, orcv.at[15])

            other(ssem, 2 * s - 2, zmod(z - s))

        @pl.when(from_above(s) & (s < 8))
        def _():
            pair = xt.at[zmod(z + s), xl]
            got(pair, ysnd.at[1, 0], yrcv.at[1, s - 1])
            ssem = osnd.at[1, lax.rem(s, 2)]

            @pl.when((s >= 3) & from_above(s - 2))
            def _():
                sent(own_block, ssem, orcv.at[15])

            other(ssem, 2 * s - 1, zmod(z + s))

    lax.fori_loop(1, 10, step, 0)

    @pl.when(z >= 8)
    def _():
        attend(z - 8, False)

    copies[15].wait()
    attended = acc[:, :128] / acc[:, 128:]
    ax[c] = (attended * ag[...]).astype(BF)
    send(ax.at[c], ax.at[c], psnd.at[1], prcv.at[1], at(z, x, o))
    ssq[p] = ssq[p] + spread(sumsq(attended), 0)
    for xx, cc in [(xf, c), (xf, o), (xr, c), (xl, c), (xr, o), (xl, o), (x, o)]:
        send(ssq.at[p], ssq.at[p], ssnd.at[0], srcv.at[0], at(z, xx, cc))
    for t in (xr, xl, x):
        for h in (0, 1):
            bpart[t, h] = pool_rows(t, h)

    def mixed_rows(t, h):
        rows = pl.ds(pl.multiple_of(t * 128, 128), 128)
        both = jnp.concatenate([ax[0, rows], ax[1, rows]], axis=1)
        return dot(both, w2[0, :, h * 512 : (h + 1) * 512])

    got(ax.at[o], psnd.at[1], prcv.at[1])
    for h in (0, 1):
        part[xf, h] = mixed_rows(xf, h).astype(BF)
    send(part.at[xf, 0], far.at[0], rsnd.at[0], rrcv.at[0], at(z, xr, c))
    send(part.at[xf, 1], far.at[1], rsnd.at[0], rrcv.at[1], at(z, xl, c))
    got(ssq.at[0:7], ssnd.at[0], srcv.at[0])
    total = ssq[0]
    for i in range(1, 8):
        total = total + ssq[i]
    factor = lax.rsqrt(total * (1.0 / 1024.0) + EPS)
    fcol[...] = jnp.concatenate([factor, jnp.zeros((120, 128), F32)], axis=0).T

    lane = lax.broadcasted_iota(jnp.int32, (128, 128), 1)

    def pick(k):
        return jnp.sum(jnp.where(lane == k, fcol[...], 0.0), axis=1, keepdims=True)

    def partial(t, hs):
        fa, fp = pick(t), pick(t + 4)
        for h in hs:
            part[t, h] = (mixed_rows(t, h) * fa + bpart[t, h] * fp).astype(BF)

    def combined(t, h):
        term = mixed_rows(t, h) + far[h].astype(F32)
        base = bpart[t, h] + fgot[h].astype(F32)
        part[t, h] = (term * pick(t) + base * pick(t + 4)).astype(BF)

    def rrows(cc):
        return pl.ds(pl.multiple_of(cc * ROWS, ROWS), ROWS)

    def to_right(h, i):
        for cc in (0, 1):
            send(part.at[xr, h, rrows(cc)], fin.at[c, i], esnd.at[0], ercv.at[0], at(z, xr, cc))

    def to_left(h, i):
        for cc in (0, 1):
            send(part.at[xl, h, rrows(cc)], fin.at[c, i], esnd.at[0], ercv.at[0], at(z, xl, cc))

    partial(xr, (1,))
    to_right(1, 2)
    partial(xl, (0,))
    to_left(0, 0)
    partial(x, (0, 1))
    send(part.at[x, :, rrows(o)], ownp, rsnd.at[1], rrcv.at[2], at(z, x, o))
    for i in (0, 1):
        got(fgot.at[i], fsnd.at[0], frcv.at[i])
    got(far.at[0], rsnd.at[0], rrcv.at[0])
    combined(xr, 0)
    to_right(0, 1)
    got(far.at[1], rsnd.at[0], rrcv.at[1])
    combined(xl, 1)
    to_left(1, 3)

    got(ownp, rsnd.at[1], rrcv.at[2])
    got(fin, esnd.at[0], ercv.at[0])
    for h in (0, 1):
        for sub in (0, 1):
            mixed = fin[h, 2 * sub].astype(F32) + fin[h, 2 * sub + 1].astype(F32)
            here = jnp.where(c == h, part[x, sub, rrows(c)].astype(F32), ownp[sub].astype(F32))
            lo = h * 1024 + sub * 512
            out[0, :, lo : lo + 512] = (mixed + here).astype(BF)

    @pl.when(rows_core)
    def _():
        sent(xt.at[z, 0:2], gsnd.at[0], grcv.at[0, 0])
        sent(nt.at[0:6], tsnd.at[0], trcv.at[0, 0])
        sent(nt.at[0:7], vsnd.at[0], vrcv.at[0])

    @pl.when(ring_core)
    def _():
        sent(xt.at[z, 0:3, 0], gsnd.at[0], grcv.at[0, 0])
        sent(nt.at[p], vsnd.at[0], vrcv.at[0])
        sent(xt.at[0:7, 0, 0], nsnd.at[0], orcv.at[15])

    sent(w2.at[:, wrows], wsnd.at[0], wrcv.at[0])
    for i in (0, 1):
        sent(px.at[c], psnd.at[i], prcv.at[i])
    sent(far, rsnd.at[0], rrcv.at[0])
    sent(ownp, rsnd.at[1], rrcv.at[2])
    sent(fpool, fsnd.at[0], frcv.at[0])
    sent(ssq.at[0:7], ssnd.at[0], srcv.at[0])
    sent(fin, esnd.at[0], ercv.at[0])

    @pl.when(z < NS - 1)
    def _():
        sent(rim, hsnd.at[0], hrcv.at[0])

    def drain(s, carry):
        odd = lax.rem(s, 2)
        other_odd = 1 - odd

        @pl.when(goes_up(s) & jnp.logical_not(goes_up(s + 2) & (s < 6)))
        def _():
            sent(xt.at[z, 0:3], usnd.at[odd], urcv.at[0, 0])

        @pl.when(goes_down(s) & (s < 7) & jnp.logical_not(goes_down(s + 2) & (s < 5)))
        def _():
            sent(xt.at[z, 0:3], dsnd.at[odd], drcv.at[0, 0])

        @pl.when(from_below(s + 1) & jnp.logical_not(from_below(s + 3) & (s < 6)))
        def _():
            sent(own, ysnd.at[0, other_odd], yrcv.at[0, 0])
            sent(own_block, osnd.at[0, other_odd], orcv.at[15])

        @pl.when(from_above(s + 1) & (s < 7) & jnp.logical_not(from_above(s + 3) & (s < 5)))
        def _():
            sent(own, ysnd.at[1, other_odd], yrcv.at[1, 0])
            sent(own_block, osnd.at[1, other_odd], orcv.at[15])

        return carry

    @pl.when(ring_core)
    def _():
        lax.fori_loop(0, 8, drain, 0)


def rope_table(length):
    halfway = 16
    inv = (1.0 / np.float32(THETA) ** (np.arange(halfway, dtype=np.float32) / np.float32(halfway))).astype(np.float32)
    angle = (np.arange(length, dtype=np.float32)[None, :] * inv[:, None]).astype(np.float32).astype(np.float64)
    return np.concatenate([np.cos(angle), np.sin(angle)], axis=0).astype(np.float32)


def local(
    tokens, input_gain, query_weight, latent_down, rotary_down, pool_down, key_up, value_up,
    query_gain, key_gain, pool_weight, pool_scale, attention_gain, pool_gain, attention_out, pool_out,
):
    width = tokens.shape[2]
    table = jnp.asarray(rope_table(NS * BLOCK))
    hbm = pl.BlockSpec(memory_space=pl.ANY)
    vmem = pl.BlockSpec(memory_space=pltpu.VMEM)
    V = pltpu.VMEM
    D = pltpu.SemaphoreType.DMA
    half = width // 2
    scratch = [
        V((ROWS, width), BF), V((1, width), F32), V((8, ROWS, width), BF), V((QK, width), BF),
        V((width, 256), BF), V((32, width), BF), V((width, 256), BF), V((256, 128), BF), V((256, 128), BF),
        V((1, QK), F32), V((1, QK), F32), V((2, 64, 64), BF), V((1, 128), F32), V((1, 128), F32),
        V((1, 128), F32), V((2, 256, half), BF), V((32, NS * BLOCK), F32),
        V((NS, NX, 2, 144, 128), BF), V((128, 256), BF), V((128, 256), BF), V((BLOCK, 128), BF),
        V((NS, 128, BLOCK), BF), V((NS, 128, BLOCK), BF), V((BLOCK, 256), F32),
        V((QK, 128), F32), V((QK, 128), F32),
        V((RIM, 128), BF), V((RIM, 128), BF), V((BLOCK + RIM, 128), F32), V((2, BLOCK, 128), BF),
        V((2, BLOCK, 128), BF), V((NX, 2, 128, half // 2), F32),
        V((8, 8, 128), F32), V((NX, 2, 128, half // 2), BF), V((2, 128, half // 2), BF),
        V((2, 4, ROWS, half // 2), BF), V((2, ROWS, half // 2), BF), V((128, 128), F32), V((2, 128, half // 2), BF), V((2, 128, half // 2), BF),
        D((17,)),
        D((2,)), D((8, 3)), D((2,)), D((7, 3)), D((2, 2)), D((2, 8)), D((1,)), D((4, 2)),
        D((2, 2)), D((19,)), D((1,)), D((2,)), D((2,)),
        D((1,)), D((2, 3)), D((1,)), D((4,)), D((1,)), D((1,)), D((1,)), D((1,)),
        D((1,)), D((1,)), D((1,)), D((1,)), D((2,)), D((3,)), D((1,)), D((2,)),
    ]
    args = (
        tokens, input_gain.reshape(1, -1), query_weight.T, latent_down, rotary_down.T, pool_down, key_up, value_up,
        query_gain.reshape(1, -1), key_gain.reshape(1, -1), pool_weight, pool_scale.reshape(1, -1),
        attention_gain.reshape(1, -1), pool_gain.reshape(1, -1), attention_out, pool_out, table,
    )
    specs = [hbm] * 17
    return pl.pallas_call(
        kernel,
        out_shape=pltpu.VMEM(tokens.shape, BF),
        in_specs=specs,
        out_specs=vmem,
        scratch_shapes=scratch,
        compiler_params=pltpu.CompilerParams(
            collective_id=0, has_side_effects=True, vmem_limit_bytes=60 * 1024 * 1024
        ),
    )(*args)


def solution(mesh):
    placed = (
        P("fs", ("sp", "tp"), None), P(), P(None, "tp"), P(), P(), P(None, "tp"), P(), P(),
        P(), P(), P(), P("tp"), P("tp"), P("tp"), P("tp", None), P("tp", None),
    )
    return jax.shard_map(
        local, mesh=mesh, in_specs=placed, out_specs=P("fs", ("sp", "tp"), None), check_vma=False
    )
```
